256 devices in a mesh: sp: 32 (over z, x), tp: 8 (over y, core).
Axes of the slice: x: 4, y: 4, z: 8, core: 2. Of those that a mesh axis runs over, the one named last changes fastest.
Arguments:
- tokens: bfloat16 [2, 6144, 4096], P(None, 'sp', 'tp'), may hold values from -12 to 12
- query_weight: bfloat16 [4096, 2048], P(None, 'tp'), may hold values from -0.09375 to 0.09375
- key_weight: bfloat16 [4096, 2048], P(None, 'tp'), may hold values from -0.09375 to 0.09375
- value_weight: bfloat16 [4096, 2048], P(None, 'tp'), may hold values from -0.09375 to 0.09375
- gate_weight: bfloat16 [4096, 2048], P(None, 'tp'), may hold values from -0.09375 to 0.09375
- beta_weight: bfloat16 [4096, 16], P(None, 'tp'), may hold values from -0.09375 to 0.09375
- decay_weight: bfloat16 [4096, 16], P(None, 'tp'), may hold values from -0.09375 to 0.09375
- beta_bias: float32 [16], P('tp'), may hold values from -6 to -3
- rate_log: float32 [16], P('tp'), may hold values from -12 to -2.5
- out_gain: float32 [128], replicated, may hold values from 0.1 to 1.9
- new_query: bfloat16 [2, 16, 128], P(None, 'tp'), may hold values from -6 to 6
- new_key: bfloat16 [2, 16, 128], P(None, 'tp'), may hold values from -6 to 6
- new_value: bfloat16 [2, 16, 128], P(None, 'tp'), may hold values from -6 to 6
- new_beta: float32 [2, 16], P(None, 'tp'), may hold values from 0.1 to 0.9
- new_decay: float32 [2, 16], P(None, 'tp'), may hold values from 0.3 to 1
Outputs:
- mixed_out: bfloat16 [2, 6144, 2048], P(None, 'sp', 'tp')
- cache: bfloat16 [2, 16, 128, 128], P(None, 'tp', 'sp')
- first_out: float32 [2, 2048], P(None, 'tp')
The draws below stay inside these ranges and needn't reach their ends.
All inputs are finite; a program needn't handle non-finite values.
Results may differ from the reference program's by a relative error of at most 0.0073.
Values may be sent and summed in bfloat16 or wider, within the bound.
A program may use at most 64 MiB of HBM per device.

```python
import jax
import jax.numpy as jnp
from jax import lax

D = 4096
HEADS = 16
HEAD = 128
BLOCK = 64
SEQS = 2
LEN = 6144


def draw_tokens(key, part):
    key_base, key_level, key_common = jax.random.split(key, 3)
    blocks = LEN // BLOCK
    base_draw = jax.random.truncated_normal(key_base, -4.0, 4.0, (SEQS, LEN, D), jnp.float32)
    level_log = jax.random.uniform(key_level, (SEQS, blocks, 1, 1), jnp.float32, -1.0, 1.0)
    common = jnp.zeros((1, 1, D), jnp.float32)
    row_scale = jnp.broadcast_to(jnp.exp(level_log), (SEQS, blocks, BLOCK, 1)).reshape(SEQS, LEN, 1)
    return ((base_draw + common) * row_scale).astype(jnp.bfloat16)


def draw_rate_log(key, part):
    key_slow, key_quick, key_pick = jax.random.split(key, 3)
    slow_rates = jnp.log(jax.random.uniform(key_slow, (HEADS,), jnp.float32, 0.2, 0.6) / LEN)
    quick_rates = jnp.log(jax.random.uniform(key_quick, (HEADS,), jnp.float32, 0.02, 0.06))
    slow_picks = jax.random.randint(key_pick, (HEADS,), 0, 2)
    return jnp.where(slow_picks == 1, slow_rates, quick_rates)


def block_scale(stream_key, shape, shards, low, largest):
    factor_of = 1.0
    for dim, shards_of in shards:
        heights = jax.random.uniform(jax.random.fold_in(jax.random.fold_in(stream_key, 6), dim), (shards_of,), jnp.float32, low / len(shards), largest / len(shards))
        factor_of = factor_of * jnp.repeat(jnp.exp(heights), shape[dim] // shards_of).reshape((-1,) + (1,) * (len(shape) - 1 - dim))
    return factor_of


def centred(key, shape, scale, reach, pieces=(), kind=jnp.bfloat16):
    array = scale * jax.random.normal(key, shape, jnp.float32)
    if pieces:
        array = array * block_scale(key, shape, pieces, -0.22, 0.18)
    return jnp.clip(array, -reach, reach).astype(kind)


def setup_inputs(seed: int = 0) -> dict:
    streams_of = jax.random.split(jax.random.key(seed), 16)
    return {
        "tokens": draw_tokens(jax.random.fold_in(streams_of[15], 71), 0),
        "query_weight": centred(streams_of[1], (D, HEADS * HEAD), D ** -0.5, 0.09375, ((1, 8),)),
        "key_weight": centred(streams_of[2], (D, HEADS * HEAD), D ** -0.5, 0.09375, ((1, 8),)),
        "value_weight": centred(streams_of[3], (D, HEADS * HEAD), D ** -0.5, 0.09375, ((1, 8),)),
        "gate_weight": centred(streams_of[4], (D, HEADS * HEAD), D ** -0.5, 0.09375, ((1, 8),)),
        "beta_weight": centred(streams_of[5], (D, HEADS), D ** -0.5, 0.09375, ((1, 8),)),
        "decay_weight": centred(streams_of[6], (D, HEADS), D ** -0.5, 0.09375, ((1, 8),)),
        "beta_bias": jnp.clip(-6.0 + 3.0 * jax.random.uniform(streams_of[7], (HEADS,), jnp.float32) ** block_scale(streams_of[7], (HEADS,), ((0, 8),), -0.2, 0.2), -6.0, -3.0),
        "rate_log": draw_rate_log(jax.random.fold_in(streams_of[15], 71), 0),
        "out_gain": jnp.clip(1.0 + 0.18 * jax.random.normal(streams_of[9], (HEAD,), jnp.float32), 0.1, 1.9),
        "new_query": centred(streams_of[10], (SEQS, HEADS, HEAD), 1.0, 6.0, ((1, 8),)),
        "new_key": centred(streams_of[11], (SEQS, HEADS, HEAD), 1.0, 6.0, ((1, 8),)),
        "new_value": centred(streams_of[12], (SEQS, HEADS, HEAD), 1.0, 6.0, ((1, 8),)),
        "new_beta": jnp.clip(0.1 + 0.79999997 * jax.random.uniform(streams_of[13], (SEQS, HEADS), jnp.float32) ** block_scale(streams_of[13], (SEQS, HEADS), ((1, 8),), -0.2, 0.2), 0.1, 0.9),
        "new_decay": jnp.clip(0.3 + 0.7 * jax.random.uniform(streams_of[14], (SEQS, HEADS), jnp.float32) ** block_scale(streams_of[14], (SEQS, HEADS), ((1, 8),), -0.2, 0.2), 0.3, 1.0),
    }


unit_floor = 1.0
norm_floor = 0.001
highest = lax.Precision.HIGHEST

def matmul(form, left, right):
    return jnp.einsum(form, left, right, precision=highest)

def unit_rows(values):
    return values * lax.rsqrt(lax.optimization_barrier(jnp.sum(values * values, axis=-1, keepdims=True)) + unit_floor)

def head_norm(values, out_gain):
    return values * lax.rsqrt(lax.optimization_barrier(jnp.mean(values * values, axis=-1, keepdims=True)) + norm_floor) * out_gain

def stored(values):
    return lax.optimization_barrier(values.astype(jnp.bfloat16)).astype(jnp.float32)

def unit_lower_inverse(lower_part):
    extent = lower_part.shape[-1]
    nilpotent = -lower_part
    inverse = jnp.eye(extent, dtype=jnp.float32) + nilpotent
    for _ in range(extent.bit_length() - 2):
        nilpotent = matmul('...ij,...jk->...ik', nilpotent, nilpotent)
        inverse = inverse + matmul('...ij,...jk->...ik', nilpotent, inverse)
    return inverse

def prepare(query_rows, key_rows, value_rows, beta_in, decay_in, beta_bias, rate_log, seq_count, length, head_count):
    extent = query_rows.shape[-1] // head_count
    blocks = length // BLOCK

    def by_head(values):
        shaped = values.reshape(seq_count, blocks, BLOCK, head_count, extent)
        return shaped.transpose(0, 3, 1, 2, 4).reshape(seq_count * head_count, blocks, BLOCK, extent)

    def by_scalar(values):
        shaped = values.reshape(seq_count, blocks, BLOCK, head_count)
        return shaped.transpose(0, 3, 1, 2).reshape(seq_count * head_count, blocks, BLOCK)
    queries = unit_rows(by_head(query_rows))
    key_unit = unit_rows(by_head(key_rows))
    values = by_head(value_rows)
    strength = by_scalar(jax.nn.sigmoid(beta_in + beta_bias))
    decays = by_scalar(-jnp.exp(rate_log) * jax.nn.softplus(decay_in))
    return (queries, key_unit, values, strength, decays)

def block_terms(queries, key_unit, values, strength, decays):
    extent = decays.shape[-1]
    cumulative = jnp.cumsum(decays, axis=-1)
    causal = jnp.tril(jnp.ones((extent, extent), bool))
    strict = jnp.tril(jnp.ones((extent, extent), bool), -1)
    spread = cumulative[..., :, None] - cumulative[..., None, :]
    weights = jnp.where(causal, jnp.exp(jnp.where(causal, spread, 0.0)), 0.0)
    key_beta = key_unit * strength[..., None]
    lower_part = jnp.where(strict, matmul('...td,...sd->...ts', key_beta, key_unit) * weights, 0.0)
    inverse = unit_lower_inverse(lower_part)
    update = matmul('...ts,...se->...te', inverse, values * strength[..., None])
    carry_w = matmul('...ts,...sd->...td', inverse, key_beta * jnp.exp(cumulative)[..., None])
    scores = matmul('...td,...sd->...ts', queries, key_unit) * weights
    query_decay = queries * jnp.exp(cumulative)[..., None]
    last_log = cumulative[..., -1]
    key_decay = key_unit * jnp.exp(last_log[..., None] - cumulative)[..., None]
    return (update, carry_w, query_decay, scores, key_decay, last_log)

def first_read(cache_whole, new_query, new_key, new_value, new_beta, new_decay, out_gain):
    seq_count, head_count, extent, _ = cache_whole.shape
    memory = lax.optimization_barrier(cache_whole).astype(jnp.float32)
    query_unit = unit_rows(new_query.astype(jnp.float32))
    key_unit = unit_rows(new_key.astype(jnp.float32))
    recall = matmul('shde,shd->she', memory, query_unit)
    retrieve = matmul('shde,shd->she', memory, key_unit)
    intersect = lax.optimization_barrier(jnp.sum(key_unit * query_unit, axis=-1))
    fresh_values = new_value.astype(jnp.float32) - new_decay[..., None] * retrieve
    read_heads = new_decay[..., None] * recall + (new_beta * intersect)[..., None] * fresh_values
    return head_norm(read_heads, out_gain).reshape(seq_count, head_count * extent)

def reference(tokens, query_weight, key_weight, value_weight, gate_weight, beta_weight, decay_weight, beta_bias, rate_log, out_gain, new_query, new_key, new_value, new_beta, new_decay):
    flat_rows = tokens.reshape(SEQS * LEN, D)

    def project(weight):
        return jnp.dot(flat_rows, weight, preferred_element_type=jnp.float32)
    query_rows = stored(project(query_weight))
    key_rows = stored(project(key_weight))
    value_rows = stored(project(value_weight))
    gate_rows = stored(project(gate_weight))
    beta_in = project(beta_weight)
    decay_in = project(decay_weight)
    prepared = prepare(query_rows, key_rows, value_rows, beta_in, decay_in, beta_bias, rate_log, SEQS, LEN, HEADS)
    block_data = block_terms(*prepared)

    def advance(state_now, inputs):
        update, carry_w, query_decay, scores, key_decay, last_log = inputs
        fresh_values = update - matmul('btd,bde->bte', carry_w, state_now)
        block_out = matmul('btd,bde->bte', query_decay, state_now) + matmul('bts,bse->bte', scores, fresh_values)
        state_next = state_now * jnp.exp(last_log)[:, None, None] + matmul('bsd,bse->bde', key_decay, fresh_values)
        return (state_next, block_out)
    inputs = tuple((jnp.moveaxis(member, 1, 0) for member in block_data))
    batch_size = SEQS * HEADS
    final_state, outputs = lax.scan(advance, jnp.zeros((batch_size, HEAD, HEAD), jnp.float32), inputs)
    heads_out = outputs.reshape(LEN // BLOCK, SEQS, HEADS, BLOCK, HEAD).transpose(1, 0, 3, 2, 4)
    heads_out = heads_out.reshape(SEQS, LEN, HEADS, HEAD)
    gate_values = gate_rows.reshape(SEQS, LEN, HEADS, HEAD)
    mixed_out = (head_norm(heads_out, out_gain) * jax.nn.silu(gate_values)).astype(jnp.bfloat16)
    mixed_out = mixed_out.reshape(SEQS, LEN, HEADS * HEAD)
    cache = final_state.reshape(SEQS, HEADS, HEAD, HEAD).astype(jnp.bfloat16)
    first_out = first_read(cache, new_query, new_key, new_value, new_beta, new_decay, out_gain)
    return (mixed_out, cache, first_out)
```

```python
import jax
import jax.numpy as jnp
from jax import lax
from jax.experimental import pallas as pl
from jax.experimental.pallas import tpu as pltpu
from jax.sharding import Mesh
from jax.sharding import PartitionSpec as P

MESH = pl.DeviceIdType.MESH
F32 = jnp.float32
BF = jnp.bfloat16
NZ, NX, NY, NC = 8, 4, 4, 2
L = 192
HALF = L // 2
E = 128
KC = 512
D = 4096
PAD = 16


def dot(a, b):
    return jnp.dot(a, b, preferred_element_type=F32)


def dot_nt(a, b):
    return lax.dot_general(a, b, (((1,), (1,)), ((), ())), preferred_element_type=F32)


def dot_tn(a, b):
    return lax.dot_general(a, b, (((0,), (0,)), ((), ())), preferred_element_type=F32)


def split3(x):
    hi = x.astype(BF)
    rest = x - hi.astype(F32)
    mid = rest.astype(BF)
    low = (rest - mid.astype(F32)).astype(BF)
    return hi, mid, low


def compose(later, earlier):
    al, rl, sl = later
    ae, re, se = earlier
    prod = dot(rl.astype(BF), jnp.concatenate([re, se], axis=1).astype(BF))
    r = al * re + ae * rl - prod[:, :E]
    s = al * se + sl - prod[:, E:]
    return al * ae, r, s


def apply_map(m, state):
    a, r, s = m
    return a * state - dot(r.astype(BF), state.astype(BF)) + s


def write_map(ref, a, r, s):
    ref[0, 0:E, :] = r.astype(BF)
    hi, mid, low = split3(a)
    row = lax.broadcasted_iota(jnp.int32, (PAD, E), 0)
    tail = jnp.where(
        row == 0,
        hi.astype(F32),
        jnp.where(row == 1, mid.astype(F32), jnp.where(row == 2, low.astype(F32), 0.0)),
    )
    ref[0, E : E + PAD, :] = tail.astype(BF)
    ref[1, 0:E, :] = s.astype(BF)


def read_map(ref):
    tail = ref[0, E : E + PAD, :].astype(F32)
    a = jnp.sum(tail, axis=0, keepdims=True)
    return a, ref[0, 0:E, :].astype(F32), ref[1, 0:E, :].astype(F32)


def kernel(
    bias_ref,
    rate_ref,
    nbeta_ref,
    ndecay_ref,
    tok_ref,
    wq_ref,
    wk_ref,
    wv_ref,
    wg_ref,
    wbd_ref,
    gain_ref,
    nq_ref,
    nk_ref,
    nv_ref,
    out_ref,
    cache_ref,
    first_ref,
    xbuf,
    wbuf,
    pj,
    lo,
    reach,
    msg,
    xin,
    zin,
    ret,
    pin,
    side,
    sin,
    wsem,
    tsem,
    ys_sem,
    yr_sem,
    fs_sem,
    fr_sem,
    ps_sem,
    pr_sem,
    xs_sem,
    xr_sem,
    zs_sem,
    zr_sem,
    rs_sem,
    rr_sem,
    ss_sem,
    sr_sem,
):
    z, x, y, c = (lax.axis_index(n) for n in ("z", "x", "y", "c"))
    yu, yd = lax.rem(y + 1, NY), lax.rem(y + NY - 1, NY)
    yf = lax.rem(y + 2, NY)
    zu, zd = lax.rem(z + 1, NZ), lax.rem(z + NZ - 1, NZ)
    other = 1 - c

    def cols(yy, cc):
        return pl.ds(pl.multiple_of((yy * NC + cc) * KC, KC), KC)

    wcopies = []
    for i, w in enumerate((wq_ref, wk_ref, wv_ref, wg_ref)):
        cp = pltpu.make_async_copy(w, wbuf.at[i], wsem.at[i])
        wcopies.append(cp)
    tcopies = []
    for s in range(2):
        cp = pltpu.make_async_copy(tok_ref.at[s], xbuf.at[s, :, cols(y, c)], tsem.at[s])
        cp.start()
        tcopies.append(cp)
    for cp in wcopies:
        cp.start()

    barrier = pltpu.get_barrier_semaphore()
    partners = [{"y": yu}, {"y": yd}, {"c": other}, {"z": zu}, {"z": zd}]
    partners += [{"x": lax.rem(x + d, NX)} for d in (1, 2, 3)]
    for p in partners:
        pl.semaphore_signal(barrier, inc=1, device_id=p, device_id_type=MESH)
    pl.semaphore_wait(barrier, len(partners))

    def ycopy(s, half, direction):
        part = xbuf.at[s, pl.ds(half * HALF, HALF), cols(y, c)]
        return pltpu.make_async_remote_copy(
            src_ref=part,
            dst_ref=part,
            send_sem=ys_sem.at[s, half, direction],
            recv_sem=yr_sem.at[s, half, direction],
            device_id={"y": yu if direction == 0 else yd},
            device_id_type=MESH,
        )

    def yarrive(s, half, direction):
        part = xbuf.at[s, pl.ds(half * HALF, HALF), cols(yd if direction == 0 else yu, c)]
        return pltpu.make_async_remote_copy(
            src_ref=part,
            dst_ref=part,
            send_sem=ys_sem.at[s, half, direction],
            recv_sem=yr_sem.at[s, half, direction],
            device_id={"y": yu if direction == 0 else yd},
            device_id_type=MESH,
        )

    def fcopy(s, direction):
        part = xbuf.at[s, pl.ds(direction * HALF, HALF), cols(yd if direction == 0 else yu, c)]
        return pltpu.make_async_remote_copy(
            src_ref=part,
            dst_ref=part,
            send_sem=fs_sem.at[s, direction],
            recv_sem=fr_sem.at[s, direction],
            device_id={"y": yu if direction == 0 else yd},
            device_id_type=MESH,
        )

    def farrive(s, direction):
        part = xbuf.at[s, pl.ds(direction * HALF, HALF), cols(yf, c)]
        return pltpu.make_async_remote_copy(
            src_ref=part,
            dst_ref=part,
            send_sem=fs_sem.at[s, direction],
            recv_sem=fr_sem.at[s, direction],
            device_id={"y": yu if direction == 0 else yd},
            device_id_type=MESH,
        )

    def pcopy(s, k, cc):
        part = xbuf.at[s, :, cols((y, yd, yu, yf)[k], cc)]
        return pltpu.make_async_remote_copy(
            src_ref=part,
            dst_ref=part,
            send_sem=ps_sem.at[s, k],
            recv_sem=pr_sem.at[s, k],
            device_id={"c": other},
            device_id_type=MESH,
        )

    def send_own(s):
        tcopies[s].wait()
        ycopy(s, 0, 0).start()
        ycopy(s, 1, 1).start()
        ycopy(s, 1, 0).start()
        ycopy(s, 0, 1).start()
        pcopy(s, 0, c).start()

    def forward(s):
        yarrive(s, 0, 0).wait_recv()
        fcopy(s, 0).start()
        yarrive(s, 1, 1).wait_recv()
        fcopy(s, 1).start()

    def finish_gather(s):
        yarrive(s, 1, 0).wait_recv()
        pcopy(s, 1, c).start()
        yarrive(s, 0, 1).wait_recv()
        pcopy(s, 2, c).start()
        farrive(s, 0).wait_recv()
        farrive(s, 1).wait_recv()
        pcopy(s, 3, c).start()
        for k in range(4):
            pcopy(s, k, other).wait_recv()

    it = lax.broadcasted_iota(jnp.int32, (L, L), 0)
    js = lax.broadcasted_iota(jnp.int32, (L, L), 1)
    lower = it >= js
    strict = it > js

    def project(s):
        def body(i, carry):
            pj[s, i] = dot(xbuf[s], wbuf[i]).astype(BF)
            return carry

        lax.fori_loop(0, 4, body, 0)

    def local_terms(s):
        bd = dot_nt(xbuf[s], wbd_ref[...])
        lane = lax.broadcasted_iota(jnp.int32, (L, PAD), 1)
        bias = jnp.where(lane == 0, bias_ref[0], jnp.where(lane == 1, bias_ref[1], 0.0))
        rate = jnp.where(lane == 2, rate_ref[0], jnp.where(lane == 3, rate_ref[1], 0.0))
        beta = jax.nn.sigmoid(bd + bias)
        soft = jnp.maximum(bd, 0.0) + jnp.log1p(jnp.exp(-jnp.abs(bd)))
        g = -jnp.exp(rate) * soft
        tri = jnp.where(lower, 1.0, 0.0).astype(BF)
        cum = sum(dot(tri, part) for part in split3(g))
        heads = range(2)
        qs = [pj[s, 0, :, h * E : (h + 1) * E] for h in heads]
        ks = [pj[s, 1, :, h * E : (h + 1) * E] for h in heads]
        vs = [pj[s, 2, :, h * E : (h + 1) * E] for h in heads]

        def scale(v):
            v = v.astype(F32)
            return lax.rsqrt(jnp.sum(v * v, axis=1, keepdims=True) + 1.0)

        rq = [scale(v) for v in qs]
        rk = [scale(v) for v in ks]
        pack = jnp.where(lane == 0, rk[0], jnp.where(lane == 1, rk[1], cum))
        eye = jnp.where(
            lax.broadcasted_iota(jnp.int32, (PAD, PAD), 0)
            == lax.broadcasted_iota(jnp.int32, (PAD, PAD), 1),
            1.0,
            0.0,
        ).astype(BF)
        rows = sum(dot_nt(eye, part) for part in split3(pack))
        amats, scores, cumc, betac = [], [], [], []
        for h in heads:
            cc = cum[:, 2 + h : 3 + h]
            bc = beta[:, h : h + 1]
            cumc.append(cc)
            betac.append(bc)
            rrow = rows[h : h + 1, :]
            crow = rows[2 + h : 3 + h, :]
            decay = jnp.exp(jnp.where(lower, cc - crow, 0.0)) * rrow
            kk = dot_nt(ks[h], ks[h])
            qk = dot_nt(qs[h], ks[h])
            amats.append(jnp.where(strict, kk * (bc * rk[h]) * decay, 0.0))
            scores.append(jnp.where(lower, qk * rq[h] * decay, 0.0).astype(BF))

        def level_mask(bit):
            return ((it >> (bit + 1)) == (js >> (bit + 1))) & ((it >> bit) != (js >> bit))

        m0 = level_mask(0)
        invs = [-jnp.where(m0, a, 0.0) for a in amats]
        for bit in range(1, 8):
            m = level_mask(bit)
            for h in heads:
                off = jnp.where(m, amats[h], 0.0)
                inv = invs[h]
                ib = inv.astype(BF)
                yy = off + dot(off.astype(BF), ib)
                invs[h] = inv - yy - dot(ib, yy.astype(BF))
        for h in heads:
            b = 2 * s + h
            kf = ks[h].astype(F32)
            ecum = jnp.exp(cumc[h])
            rhs = jnp.concatenate(
                [kf * (betac[h] * rk[h] * ecum), vs[h].astype(F32) * betac[h]], axis=1
            )
            sol = rhs + dot(invs[h].astype(BF), rhs.astype(BF))
            sb = sol.astype(BF)
            last = cumc[h][L - 1 : L, :]
            kd = kf * (rk[h] * jnp.exp(last - cumc[h]))
            rs = dot_tn(kd.astype(BF), sb)
            sx = dot(scores[h], sb)
            a = jnp.broadcast_to(jnp.exp(last), (1, E))
            write_map(msg.at[b], a, rs[:, :E], rs[:, E:])
            lo[b] = sx[:, E:]
            qd = qs[h].astype(F32) * (rq[h] * ecum)
            reach[b] = (qd - sx[:, :E]).astype(BF)

    def xcopy(b, src_x):
        return pltpu.make_async_remote_copy(
            src_ref=msg.at[b],
            dst_ref=xin.at[src_x],
            send_sem=xs_sem.at[b],
            recv_sem=xr_sem.at[src_x],
            device_id={"x": b},
            device_id_type=MESH,
        )

    def xlocal(b):
        return pltpu.make_async_copy(msg.at[b], xin.at[b], xs_sem.at[b])

    def xsend(b):
        @pl.when(x != b)
        def _():
            xcopy(b, x).start()

        @pl.when(x == b)
        def _():
            xlocal(b).start()

    send_own(0)
    forward(0)
    send_own(1)
    finish_gather(0)
    for cp in wcopies:
        cp.wait()
    project(0)
    forward(1)
    local_terms(0)
    xsend(0)
    xsend(1)
    finish_gather(1)
    project(1)
    local_terms(1)
    xsend(2)
    xsend(3)

    for j in range(NX):

        @pl.when(x != j)
        def _():
            xcopy(j, j).wait_recv()

        @pl.when(x == j)
        def _():
            xlocal(j).wait()

    maps = [read_map(xin.at[j]) for j in range(NX)]
    m10 = compose(maps[1], maps[0])
    m32 = compose(maps[3], maps[2])
    total = compose(m32, m10)
    write_map(zin.at[z], *total)

    def zslot(step, direction):
        if direction == 0:
            return lax.rem(z + NZ - (step - 1), NZ)
        return lax.rem(z + (step - 1), NZ)

    def zcopy(step, piece, direction, slot):
        part = zin.at[slot, piece]
        return pltpu.make_async_remote_copy(
            src_ref=part,
            dst_ref=part,
            send_sem=zs_sem.at[step - 1, piece, direction],
            recv_sem=zr_sem.at[step - 1, piece, direction],
            device_id={"z": zu if direction == 0 else zd},
            device_id_type=MESH,
        )

    for step in range(1, 5):
        for piece in range(2):
            for direction in range(2):
                if direction == 1 and step > 3:
                    continue
                slot = zslot(step, direction)
                if step > 1:
                    zcopy(step - 1, piece, direction, slot).wait_recv()
                zcopy(step, piece, direction, slot).start()
    m210 = compose(maps[2], m10)
    for piece in range(2):
        zcopy(3, piece, 1, zslot(4, 1)).wait_recv()
        zcopy(4, piece, 0, zslot(5, 0)).wait_recv()

    state = jnp.zeros((E, E), F32)
    here = state
    for k in range(NZ):
        here = jnp.where(z == k, state, here)
        m = read_map(zin.at[k])
        state = m[2] if k == 0 else apply_map(m, state)
    starts = [here] + [apply_map(m, here) for m in (maps[0], m10, m210)]

    def rcopy(j, b):
        return pltpu.make_async_remote_copy(
            src_ref=ret.at[j],
            dst_ref=pin.at[b],
            send_sem=rs_sem.at[j],
            recv_sem=rr_sem.at[b],
            device_id={"x": j},
            device_id_type=MESH,
        )

    def rlocal(j):
        return pltpu.make_async_copy(ret.at[j], pin.at[j], rs_sem.at[j])

    def scopy(j, b):
        return pltpu.make_async_remote_copy(
            src_ref=side.at[j],
            dst_ref=sin.at[b],
            send_sem=ss_sem.at[j],
            recv_sem=sr_sem.at[b],
            device_id={"x": j},
            device_id_type=MESH,
        )

    def slocal(j):
        return pltpu.make_async_copy(side.at[j], sin.at[j], ss_sem.at[j])

    for j in range(NX):
        ret[j] = starts[j].astype(BF)

        @pl.when(x != j)
        def _():
            rcopy(j, x).start()

        @pl.when(x == j)
        def _():
            rlocal(j).start()

    memory = state.astype(BF)

    def pick(ref):
        row = ref[0, 0:1, :].astype(F32)
        for b in range(1, 4):
            row = jnp.where(x == b, ref[b // 2, b % 2 : b % 2 + 1, :].astype(F32), row)
        return row

    def pick_scalar(ref):
        value = ref[0, 0]
        for b in range(1, 4):
            value = jnp.where(x == b, ref[b // 2, b % 2], value)
        return value

    def unit(v):
        return v * lax.rsqrt(jnp.sum(v * v, axis=1, keepdims=True) + 1.0)

    qn, kn, nv = unit(pick(nq_ref)), unit(pick(nk_ref)), pick(nv_ref)
    nbeta, ndecay = pick_scalar(nbeta_ref), pick_scalar(ndecay_ref)
    row8 = lax.broadcasted_iota(jnp.int32, (PAD, E), 0)
    probe = jnp.where(row8 == 0, qn, jnp.where(row8 == 1, kn, 0.0))
    seen = sum(dot(part, memory) for part in split3(probe))
    recall, retrieve = seen[0:1, :], seen[1:2, :]
    intersect = jnp.sum(kn * qn, axis=1, keepdims=True)
    fresh = nv - ndecay * retrieve
    read = ndecay * recall + (nbeta * intersect) * fresh
    gain = gain_ref[...]
    first = read * lax.rsqrt(jnp.mean(read * read, axis=1, keepdims=True) + 0.001) * gain

    memf = memory.astype(F32)
    mine = memf[0:16, :]
    for k in range(1, NZ):
        mine = jnp.where(z == k, memf[16 * k : 16 * k + 16, :], mine)
    for j in range(NX):
        side[j, 0:4, :] = mine[4 * j : 4 * j + 4, :]
        side[j, 4:8, :] = jnp.broadcast_to(first, (4, E))

        @pl.when(x != j)
        def _():
            scopy(j, x).start()

        @pl.when(x == j)
        def _():
            slocal(j).start()

    for b in range(4):

        @pl.when(x != b)
        def _():
            rcopy(b, b).wait_recv()

        @pl.when(x == b)
        def _():
            rlocal(b).wait()

    for b in range(4):
        s, h = b // 2, b % 2
        o = lo[b] + dot(reach[b], pin[b])
        gate = pj[s, 3, :, h * E : (h + 1) * E].astype(F32)
        norm = lax.rsqrt(jnp.mean(o * o, axis=1, keepdims=True) + 0.001)
        out_ref[s, :, h * E : (h + 1) * E] = (
            o * norm * gain * (gate * jax.nn.sigmoid(gate))
        ).astype(BF)

    for b in range(4):

        @pl.when(x != b)
        def _():
            scopy(b, b).wait_recv()

        @pl.when(x == b)
        def _():
            slocal(b).wait()

    for b in range(4):
        s, h = b // 2, b % 2
        cache_ref[s, h] = sin[b, 0:4, :].astype(BF)
        first_ref[s : s + 1, h * E : (h + 1) * E] = sin[b, 4:5, :]

    for s in range(2):
        for half in range(2):
            for direction in range(2):
                ycopy(s, half, direction).wait_send()
        for direction in range(2):
            fcopy(s, direction).wait_send()
        for k in range(4):
            pcopy(s, k, c).wait_send()
    for j in range(NX):

        @pl.when(x != j)
        def _():
            xcopy(j, x).wait_send()
            rcopy(j, x).wait_send()
            scopy(j, x).wait_send()

    for step in range(1, 5):
        for piece in range(2):
            for direction in range(2):
                if direction == 1 and step > 3:
                    continue
                zcopy(step, piece, direction, zslot(step, direction)).wait_send()


def shards(
    tokens,
    query_weight,
    key_weight,
    value_weight,
    gate_weight,
    beta_weight,
    decay_weight,
    beta_bias,
    rate_log,
    out_gain,
    new_query,
    new_key,
    new_value,
    new_beta,
    new_decay,
):
    wbd = jnp.concatenate(
        [beta_weight.T, decay_weight.T, jnp.zeros((PAD - 4, D), BF)], axis=0
    )
    smem = pl.BlockSpec(memory_space=pltpu.SMEM)
    vmem = pl.BlockSpec(memory_space=pltpu.VMEM)
    hbm = pl.BlockSpec(memory_space=pl.ANY)
    dma = pltpu.SemaphoreType.DMA
    out = pl.pallas_call(
        kernel,
        out_shape=(
            jax.ShapeDtypeStruct((2, L, 2 * E), BF),
            jax.ShapeDtypeStruct((2, 2, 4, E), BF),
            jax.ShapeDtypeStruct((2, 2 * E), F32),
        ),
        in_specs=[smem] * 4 + [hbm] * 5 + [vmem] * 5,
        out_specs=(vmem, vmem, vmem),
        scratch_shapes=[
            pltpu.VMEM((2, L, D), BF),
            pltpu.VMEM((4, D, 2 * E), BF),
            pltpu.VMEM((2, 4, L, 2 * E), BF),
            pltpu.VMEM((4, L, E), F32),
            pltpu.VMEM((4, L, E), BF),
            pltpu.VMEM((4, 2, E + PAD, E), BF),
            pltpu.VMEM((4, 2, E + PAD, E), BF),
            pltpu.VMEM((NZ, 2, E + PAD, E), BF),
            pltpu.VMEM((4, E, E), BF),
            pltpu.VMEM((4, E, E), BF),
            pltpu.VMEM((4, 8, E), F32),
            pltpu.VMEM((4, 8, E), F32),
            dma((4,)),
            dma((2,)),
            dma((2, 2, 2)),
            dma((2, 2, 2)),
            dma((2, 2)),
            dma((2, 2)),
            dma((2, 4)),
            dma((2, 4)),
            dma((4,)),
            dma((4,)),
            dma((4, 2, 2)),
            dma((4, 2, 2)),
            dma((4,)),
            dma((4,)),
            dma((4,)),
            dma((4,)),
        ],
        compiler_params=pltpu.CompilerParams(
            collective_id=0, has_side_effects=True, vmem_limit_bytes=60 * 1024 * 1024
        ),
        name="delta_all",
    )(
        beta_bias,
        rate_log,
        new_beta,
        new_decay,
        tokens,
        query_weight,
        key_weight,
        value_weight,
        gate_weight,
        wbd,
        out_gain.reshape(1, E),
        new_query,
        new_key,
        new_value,
    )
    return out


def solution(mesh):
    torus = Mesh(mesh.devices.reshape(NZ, NX, NY, NC), ("z", "x", "y", "c"))
    sp, tp = ("z", "x"), ("y", "c")
    in_specs = (
        P(None, sp, tp),
        P(None, tp),
        P(None, tp),
        P(None, tp),
        P(None, tp),
        P(None, tp),
        P(None, tp),
        P(tp),
        P(tp),
        P(),
        P(None, tp, None),
        P(None, tp, None),
        P(None, tp, None),
        P(None, tp),
        P(None, tp),
    )
    out_specs = (P(None, sp, tp), P(None, tp, sp, None), P(None, tp))
    return jax.shard_map(
        shards, mesh=torus, in_specs=in_specs, out_specs=out_specs, check_vma=False
    )
```

```python
import jax
import jax.numpy as jnp
from jax import lax
from jax.experimental import pallas as pl
from jax.experimental.pallas import tpu as pltpu
from jax.sharding import Mesh
from jax.sharding import PartitionSpec as P

MESH = pl.DeviceIdType.MESH
F32 = jnp.float32
BF = jnp.bfloat16
NZ, NX, NY, NC = 8, 4, 4, 2
L = 192
HALF = L // 2
E = 128
KC = 512
D = 4096
PAD = 16


def dot(a, b):
    return jnp.dot(a, b, preferred_element_type=F32)


def dot_nt(a, b):
    return lax.dot_general(a, b, (((1,), (1,)), ((), ())), preferred_element_type=F32)


def dot_tn(a, b):
    return lax.dot_general(a, b, (((0,), (0,)), ((), ())), preferred_element_type=F32)


def split3(x):
    hi = x.astype(BF)
    rest = x - hi.astype(F32)
    mid = rest.astype(BF)
    low = (rest - mid.astype(F32)).astype(BF)
    return hi, mid, low


def compose(later, earlier):
    al, rl, sl = later
    ae, re, se = earlier
    prod = dot(rl.astype(BF), jnp.concatenate([re, se], axis=1).astype(BF))
    r = al * re + ae * rl - prod[:, :E]
    s = al * se + sl - prod[:, E:]
    return al * ae, r, s


def apply_map(m, state):
    a, r, s = m
    return a * state - dot(r.astype(BF), state.astype(BF)) + s


def write_map(ref, a, r, s):
    ref[0, 0:E, :] = r.astype(BF)
    hi, mid, low = split3(a)
    row = lax.broadcasted_iota(jnp.int32, (PAD, E), 0)
    tail = jnp.where(
        row == 0,
        hi.astype(F32),
        jnp.where(row == 1, mid.astype(F32), jnp.where(row == 2, low.astype(F32), 0.0)),
    )
    ref[0, E : E + PAD, :] = tail.astype(BF)
    ref[1, 0:E, :] = s.astype(BF)


def read_map(ref):
    tail = ref[0, E : E + PAD, :].astype(F32)
    a = jnp.sum(tail, axis=0, keepdims=True)
    return a, ref[0, 0:E, :].astype(F32), ref[1, 0:E, :].astype(F32)


def kernel(
    bias_ref,
    rate_ref,
    nbeta_ref,
    ndecay_ref,
    tok_ref,
    wq_ref,
    wk_ref,
    wv_ref,
    wg_ref,
    wb_ref,
    wd_ref,
    gain_ref,
    nq_ref,
    nk_ref,
    nv_ref,
    out_ref,
    cache_ref,
    first_ref,
    xbuf,
    wbuf,
    pj,
    acc,
    wbd,
    lo,
    reach,
    sols,
    msg,
    xin,
    zin,
    ret,
    pin,
    side,
    sin,
    wsem,
    tsem,
    ys_sem,
    yr_sem,
    fs_sem,
    fr_sem,
    ps_sem,
    pr_sem,
    xs_sem,
    xr_sem,
    zs_sem,
    zr_sem,
    rs_sem,
    rr_sem,
    ss_sem,
    sr_sem,
):
    z, x, y, c = (lax.axis_index(n) for n in ("z", "x", "y", "c"))
    yu, yd = lax.rem(y + 1, NY), lax.rem(y + NY - 1, NY)
    yf = lax.rem(y + 2, NY)
    zu, zd = lax.rem(z + 1, NZ), lax.rem(z + NZ - 1, NZ)
    other = 1 - c

    def cols(yy, cc):
        return pl.ds(pl.multiple_of((yy * NC + cc) * KC, KC), KC)

    wcopies = []
    for i, w in enumerate((wq_ref, wk_ref, wv_ref, wg_ref)):
        cp = pltpu.make_async_copy(w, wbuf.at[i], wsem.at[i])
        wcopies.append(cp)
    tcopies = []
    for s in range(2):
        cp = pltpu.make_async_copy(tok_ref.at[s], xbuf.at[s, :, cols(y, c)], tsem.at[s])
        cp.start()
        tcopies.append(cp)
    for cp in wcopies:
        cp.start()

    wbd[...] = jnp.concatenate(
        [wb_ref[...].astype(F32), wd_ref[...].astype(F32), jnp.zeros((PAD - 4, D), F32)], axis=0
    ).astype(BF)

    barrier = pltpu.get_barrier_semaphore()
    partners = [{"y": yu}, {"y": yd}, {"c": other}, {"z": zu}, {"z": zd}]
    partners += [{"x": lax.rem(x + d, NX)} for d in (1, 2, 3)]
    for p in partners:
        pl.semaphore_signal(barrier, inc=1, device_id=p, device_id_type=MESH)
    pl.semaphore_wait(barrier, len(partners))

    def ycopy(s, half, direction):
        part = xbuf.at[s, pl.ds(half * HALF, HALF), cols(y, c)]
        return pltpu.make_async_remote_copy(
            src_ref=part,
            dst_ref=part,
            send_sem=ys_sem.at[s, half, direction],
            recv_sem=yr_sem.at[s, half, direction],
            device_id={"y": yu if direction == 0 else yd},
            device_id_type=MESH,
        )

    def yarrive(s, half, direction):
        part = xbuf.at[s, pl.ds(half * HALF, HALF), cols(yd if direction == 0 else yu, c)]
        return pltpu.make_async_remote_copy(
            src_ref=part,
            dst_ref=part,
            send_sem=ys_sem.at[s, half, direction],
            recv_sem=yr_sem.at[s, half, direction],
            device_id={"y": yu if direction == 0 else yd},
            device_id_type=MESH,
        )

    def fcopy(s, direction):
        part = xbuf.at[s, pl.ds(direction * HALF, HALF), cols(yd if direction == 0 else yu, c)]
        return pltpu.make_async_remote_copy(
            src_ref=part,
            dst_ref=part,
            send_sem=fs_sem.at[s, direction],
            recv_sem=fr_sem.at[s, direction],
            device_id={"y": yu if direction == 0 else yd},
            device_id_type=MESH,
        )

    def farrive(s, direction):
        part = xbuf.at[s, pl.ds(direction * HALF, HALF), cols(yf, c)]
        return pltpu.make_async_remote_copy(
            src_ref=part,
            dst_ref=part,
            send_sem=fs_sem.at[s, direction],
            recv_sem=fr_sem.at[s, direction],
            device_id={"y": yu if direction == 0 else yd},
            device_id_type=MESH,
        )

    def pcopy(s, k, cc):
        part = xbuf.at[s, :, cols((y, yd, yu, yf)[k], cc)]
        return pltpu.make_async_remote_copy(
            src_ref=part,
            dst_ref=part,
            send_sem=ps_sem.at[s, k],
            recv_sem=pr_sem.at[s, k],
            device_id={"c": other},
            device_id_type=MESH,
        )

    def send_own(s):
        tcopies[s].wait()
        ycopy(s, 0, 0).start()
        ycopy(s, 1, 1).start()
        ycopy(s, 1, 0).start()
        ycopy(s, 0, 1).start()
        pcopy(s, 0, c).start()

    def forward(s):
        yarrive(s, 0, 0).wait_recv()
        fcopy(s, 0).start()
        yarrive(s, 1, 1).wait_recv()
        fcopy(s, 1).start()

    def finish_near(s):
        yarrive(s, 1, 0).wait_recv()
        pcopy(s, 1, c).start()
        yarrive(s, 0, 1).wait_recv()
        pcopy(s, 2, c).start()
        for k in range(3):
            pcopy(s, k, other).wait_recv()

    def finish_far(s):
        farrive(s, 0).wait_recv()
        farrive(s, 1).wait_recv()
        pcopy(s, 3, c).start()
        pcopy(s, 3, other).wait_recv()

    it = lax.broadcasted_iota(jnp.int32, (L, L), 0)
    js = lax.broadcasted_iota(jnp.int32, (L, L), 1)
    lower = it >= js
    strict = it > js

    def project(s, which):
        for i in which:
            pj[s, i] = dot(xbuf[s], wbuf[i]).astype(BF)

    def small(s):
        return dot_nt(xbuf[s], wbd[...])

    def chip(yy):
        return pl.ds(pl.multiple_of(yy * NC * KC, NC * KC), NC * KC)

    def near(s):
        for n, i in enumerate((1, 2)):
            acc[n] = sum(dot(xbuf[s, :, chip(q)], wbuf[i, chip(q), :]) for q in (y, yd, yu))
        return sum(dot_nt(xbuf[s, :, chip(q)], wbd[:, chip(q)]) for q in (y, yd, yu))

    def far(s, part):
        for n, i in enumerate((1, 2)):
            pj[s, i] = (acc[n] + dot(xbuf[s, :, chip(yf)], wbuf[i, chip(yf), :])).astype(BF)
        return part + dot_nt(xbuf[s, :, chip(yf)], wbd[:, chip(yf)])

    heads = range(2)

    def scale(v):
        v = v.astype(F32)
        return lax.rsqrt(jnp.sum(v * v, axis=1, keepdims=True) + 1.0)

    def head_of(s, i, h):
        return pj[s, i, :, h * E : (h + 1) * E]

    def chain_terms(s, bd):
        lane = lax.broadcasted_iota(jnp.int32, (L, PAD), 1)
        bias = jnp.where(lane == 0, bias_ref[0], jnp.where(lane == 1, bias_ref[1], 0.0))
        rate = jnp.where(lane == 2, rate_ref[0], jnp.where(lane == 3, rate_ref[1], 0.0))
        beta = jax.nn.sigmoid(bd + bias)
        soft = jnp.maximum(bd, 0.0) + jnp.log1p(jnp.exp(-jnp.abs(bd)))
        g = -jnp.exp(rate) * soft
        tri = jnp.where(lower, 1.0, 0.0).astype(BF)
        cum = sum(dot(tri, part) for part in split3(g))
        ks = [head_of(s, 1, h) for h in heads]
        vs = [head_of(s, 2, h) for h in heads]
        rk = [scale(v) for v in ks]
        pack = jnp.where(lane == 0, rk[0], jnp.where(lane == 1, rk[1], cum))
        eye = jnp.where(
            lax.broadcasted_iota(jnp.int32, (PAD, PAD), 0)
            == lax.broadcasted_iota(jnp.int32, (PAD, PAD), 1),
            1.0,
            0.0,
        ).astype(BF)
        rows = sum(dot_nt(eye, part) for part in split3(pack))
        amats, cumc, betac = [], [], []
        for h in heads:
            cc = cum[:, 2 + h : 3 + h]
            bc = beta[:, h : h + 1]
            cumc.append(cc)
            betac.append(bc)
            rrow = rows[h : h + 1, :]
            crow = rows[2 + h : 3 + h, :]
            decay = jnp.exp(jnp.where(lower, cc - crow, 0.0)) * rrow
            kk = dot_nt(ks[h], ks[h])
            amats.append(jnp.where(strict, kk * (bc * rk[h]) * decay, 0.0))

        def level_mask(bit):
            return ((it >> (bit + 1)) == (js >> (bit + 1))) & ((it >> bit) != (js >> bit))

        m0 = level_mask(0)
        invs = [-jnp.where(m0, a, 0.0) for a in amats]
        for bit in range(1, 8):
            m = level_mask(bit)
            for h in heads:
                off = jnp.where(m, amats[h], 0.0)
                inv = invs[h]
                ib = inv.astype(BF)
                yy = off + dot(off.astype(BF), ib)
                invs[h] = inv - yy - dot(ib, yy.astype(BF))
        for h in heads:
            b = 2 * s + h
            kf = ks[h].astype(F32)
            ecum = jnp.exp(cumc[h])
            rhs = jnp.concatenate(
                [kf * (betac[h] * rk[h] * ecum), vs[h].astype(F32) * betac[h]], axis=1
            )
            sol = rhs + dot(invs[h].astype(BF), rhs.astype(BF))
            sb = sol.astype(BF)
            last = cumc[h][L - 1 : L, :]
            kd = kf * (rk[h] * jnp.exp(last - cumc[h]))
            rs = dot_tn(kd.astype(BF), sb)
            a = jnp.broadcast_to(jnp.exp(last), (1, E))
            write_map(msg.at[b], a, rs[:, :E], rs[:, E:])
            sols[b] = sb
        return cumc, rows

    def out_terms(s, cumc, rows):
        for h in heads:
            b = 2 * s + h
            q, k = head_of(s, 0, h), head_of(s, 1, h)
            rq = scale(q)
            cc = cumc[h]
            decay = jnp.exp(jnp.where(lower, cc - rows[2 + h : 3 + h, :], 0.0)) * rows[h : h + 1, :]
            score = jnp.where(lower, dot_nt(q, k) * rq * decay, 0.0).astype(BF)
            sx = dot(score, sols[b])
            lo[b] = sx[:, E:]
            qd = q.astype(F32) * (rq * jnp.exp(cc))
            reach[b] = (qd - sx[:, :E]).astype(BF)

    def xcopy(b, src_x):
        return pltpu.make_async_remote_copy(
            src_ref=msg.at[b],
            dst_ref=xin.at[src_x],
            send_sem=xs_sem.at[b],
            recv_sem=xr_sem.at[src_x],
            device_id={"x": b},
            device_id_type=MESH,
        )

    def xlocal(b):
        return pltpu.make_async_copy(msg.at[b], xin.at[b], xs_sem.at[b])

    def xsend(b):
        @pl.when(x != b)
        def _():
            xcopy(b, x).start()

        @pl.when(x == b)
        def _():
            xlocal(b).start()

    send_own(0)
    forward(0)
    send_own(1)
    finish_near(0)
    finish_far(0)
    for cp in wcopies:
        cp.wait()
    project(0, (1, 2))
    forward(1)
    kept0 = chain_terms(0, small(0))
    xsend(0)
    xsend(1)
    project(0, (0, 3))
    out_terms(0, *kept0)
    finish_near(1)
    part = near(1)
    finish_far(1)
    kept1 = chain_terms(1, far(1, part))
    xsend(2)
    xsend(3)
    project(1, (0, 3))
    out_terms(1, *kept1)

    for j in range(NX):

        @pl.when(x != j)
        def _():
            xcopy(j, j).wait_recv()

        @pl.when(x == j)
        def _():
            xlocal(j).wait()

    maps = [read_map(xin.at[j]) for j in range(NX)]
    m10 = compose(maps[1], maps[0])
    m32 = compose(maps[3], maps[2])
    total = compose(m32, m10)
    write_map(zin.at[z], *total)

    def zslot(step, direction):
        if direction == 0:
            return lax.rem(z + NZ - (step - 1), NZ)
        return lax.rem(z + (step - 1), NZ)

    def zcopy(step, piece, direction, slot):
        part = zin.at[slot, piece]
        return pltpu.make_async_remote_copy(
            src_ref=part,
            dst_ref=part,
            send_sem=zs_sem.at[step - 1, piece, direction],
            recv_sem=zr_sem.at[step - 1, piece, direction],
            device_id={"z": zu if direction == 0 else zd},
            device_id_type=MESH,
        )

    def zmap(k, valid):
        a, r, v = read_map(zin.at[lax.rem(k + NZ, NZ)])
        return (
            jnp.where(valid, a, 1.0),
            jnp.where(valid, r, 0.0),
            jnp.where(valid, v, 0.0),
        )

    behind = None
    early = None
    for step in range(1, 6):
        for piece in range(2):
            for direction in range(2):
                slot = zslot(step, direction)
                if step > 1 and step - 1 <= 4 - direction:
                    zcopy(step - 1, piece, direction, slot).wait_recv()
                if step <= 4 - direction:
                    zcopy(step, piece, direction, slot).start()
        if step == 1:
            m210 = compose(maps[2], m10)
            continue
        dist = step - 1
        if dist <= 3:
            found = zmap(z + dist, z + dist >= NZ)
            early = found[2] if early is None else apply_map(found, early)
            found = zmap(z - dist, z - dist >= 0)
            behind = found if behind is None else compose(behind, found)
        else:
            early = apply_map(zmap(z - dist, z - dist >= 0), early)
    here = apply_map(behind, early)
    starts = [here] + [apply_map(m, here) for m in (maps[0], m10, m210)]

    def rcopy(j, b):
        return pltpu.make_async_remote_copy(
            src_ref=ret.at[j],
            dst_ref=pin.at[b],
            send_sem=rs_sem.at[j],
            recv_sem=rr_sem.at[b],
            device_id={"x": j},
            device_id_type=MESH,
        )

    def rlocal(j):
        return pltpu.make_async_copy(ret.at[j], pin.at[j], rs_sem.at[j])

    def scopy(j, b):
        return pltpu.make_async_remote_copy(
            src_ref=side.at[j],
            dst_ref=sin.at[b],
            send_sem=ss_sem.at[j],
            recv_sem=sr_sem.at[b],
            device_id={"x": j},
            device_id_type=MESH,
        )

    def slocal(j):
        return pltpu.make_async_copy(side.at[j], sin.at[j], ss_sem.at[j])

    for j in range(NX):
        ret[j] = starts[j].astype(BF)

        @pl.when(x != j)
        def _():
            rcopy(j, x).start()

        @pl.when(x == j)
        def _():
            rlocal(j).start()

    state = read_map(zin.at[0])[2]
    for k in range(1, NZ):
        state = apply_map(read_map(zin.at[k]), state)

    memory = state.astype(BF)

    def pick(ref):
        row = ref[0, 0:1, :].astype(F32)
        for b in range(1, 4):
            row = jnp.where(x == b, ref[b // 2, b % 2 : b % 2 + 1, :].astype(F32), row)
        return row

    def pick_scalar(ref):
        value = ref[0, 0]
        for b in range(1, 4):
            value = jnp.where(x == b, ref[b // 2, b % 2], value)
        return value

    def unit(v):
        return v * lax.rsqrt(jnp.sum(v * v, axis=1, keepdims=True) + 1.0)

    qn, kn, nv = unit(pick(nq_ref)), unit(pick(nk_ref)), pick(nv_ref)
    nbeta, ndecay = pick_scalar(nbeta_ref), pick_scalar(ndecay_ref)
    row8 = lax.broadcasted_iota(jnp.int32, (PAD, E), 0)
    probe = jnp.where(row8 == 0, qn, jnp.where(row8 == 1, kn, 0.0))
    seen = sum(dot(part, memory) for part in split3(probe))
    recall, retrieve = seen[0:1, :], seen[1:2, :]
    intersect = jnp.sum(kn * qn, axis=1, keepdims=True)
    fresh = nv - ndecay * retrieve
    read = ndecay * recall + (nbeta * intersect) * fresh
    gain = gain_ref[...]
    first = read * lax.rsqrt(jnp.mean(read * read, axis=1, keepdims=True) + 0.001) * gain

    memf = memory.astype(F32)
    mine = memf[0:16, :]
    for k in range(1, NZ):
        mine = jnp.where(z == k, memf[16 * k : 16 * k + 16, :], mine)
    for j in range(NX):
        side[j, 0:4, :] = mine[4 * j : 4 * j + 4, :]
        side[j, 4:8, :] = jnp.broadcast_to(first, (4, E))

        @pl.when(x != j)
        def _():
            scopy(j, x).start()

        @pl.when(x == j)
        def _():
            slocal(j).start()

    for b in range(4):

        @pl.when(x != b)
        def _():
            rcopy(b, b).wait_recv()

        @pl.when(x == b)
        def _():
            rlocal(b).wait()

    for b in range(4):
        s, h = b // 2, b % 2
        o = lo[b] + dot(reach[b], pin[b])
        gate = pj[s, 3, :, h * E : (h + 1) * E].astype(F32)
        norm = lax.rsqrt(jnp.mean(o * o, axis=1, keepdims=True) + 0.001)
        out_ref[s, :, h * E : (h + 1) * E] = (
            o * norm * gain * (gate * jax.nn.sigmoid(gate))
        ).astype(BF)

    for b in range(4):

        @pl.when(x != b)
        def _():
            scopy(b, b).wait_recv()

        @pl.when(x == b)
        def _():
            slocal(b).wait()

    for b in range(4):
        s, h = b // 2, b % 2
        cache_ref[s, h] = sin[b, 0:4, :].astype(BF)
        first_ref[s : s + 1, h * E : (h + 1) * E] = sin[b, 4:5, :]

    for s in range(2):
        for half in range(2):
            for direction in range(2):
                ycopy(s, half, direction).wait_send()
        for direction in range(2):
            fcopy(s, direction).wait_send()
        for k in range(4):
            pcopy(s, k, c).wait_send()
    for j in range(NX):

        @pl.when(x != j)
        def _():
            xcopy(j, x).wait_send()
            rcopy(j, x).wait_send()
            scopy(j, x).wait_send()

    for step in range(1, 5):
        for piece in range(2):
            for direction in range(2):
                if direction == 1 and step > 3:
                    continue
                zcopy(step, piece, direction, zslot(step, direction)).wait_send()


def hand_over(mixed_in, cache_in, first_in, mixed_out, cache_out, first_out):
    mixed_out[...] = mixed_in[...]
    cache_out[...] = cache_in[...]
    first_out[...] = first_in[...]


def shards(
    tokens,
    query_weight,
    key_weight,
    value_weight,
    gate_weight,
    beta_weight,
    decay_weight,
    beta_bias,
    rate_log,
    out_gain,
    new_query,
    new_key,
    new_value,
    new_beta,
    new_decay,
):
    smem = pl.BlockSpec(memory_space=pltpu.SMEM)
    vmem = pl.BlockSpec(memory_space=pltpu.VMEM)
    hbm = pl.BlockSpec(memory_space=pl.ANY)
    dma = pltpu.SemaphoreType.DMA
    out = pl.pallas_call(
        kernel,
        out_shape=(
            jax.ShapeDtypeStruct((2, L, 2 * E), BF),
            jax.ShapeDtypeStruct((2, 2, 4, E), BF),
            jax.ShapeDtypeStruct((2, 2 * E), F32),
        ),
        in_specs=[smem] * 4 + [hbm] * 5 + [vmem] * 6,
        out_specs=(vmem, vmem, vmem),
        scratch_shapes=[
            pltpu.VMEM((2, L, D), BF),
            pltpu.VMEM((4, D, 2 * E), BF),
            pltpu.VMEM((2, 4, L, 2 * E), BF),
            pltpu.VMEM((2, L, 2 * E), F32),
            pltpu.VMEM((PAD, D), BF),
            pltpu.VMEM((4, L, E), F32),
            pltpu.VMEM((4, L, E), BF),
            pltpu.VMEM((4, L, 2 * E), BF),
            pltpu.VMEM((4, 2, E + PAD, E), BF),
            pltpu.VMEM((4, 2, E + PAD, E), BF),
            pltpu.VMEM((NZ, 2, E + PAD, E), BF),
            pltpu.VMEM((4, E, E), BF),
            pltpu.VMEM((4, E, E), BF),
            pltpu.VMEM((4, 8, E), F32),
            pltpu.VMEM((4, 8, E), F32),
            dma((4,)),
            dma((2,)),
            dma((2, 2, 2)),
            dma((2, 2, 2)),
            dma((2, 2)),
            dma((2, 2)),
            dma((2, 4)),
            dma((2, 4)),
            dma((4,)),
            dma((4,)),
            dma((4, 2, 2)),
            dma((4, 2, 2)),
            dma((4,)),
            dma((4,)),
            dma((4,)),
            dma((4,)),
        ],
        compiler_params=pltpu.CompilerParams(
            collective_id=0, has_side_effects=True, vmem_limit_bytes=60 * 1024 * 1024
        ),
        name="delta_all",
    )(
        beta_bias,
        rate_log,
        new_beta,
        new_decay,
        tokens,
        query_weight,
        key_weight,
        value_weight,
        gate_weight,
        beta_weight.T,
        decay_weight.T,
        out_gain.reshape(1, E),
        new_query,
        new_key,
        new_value,
    )
    return pl.pallas_call(
        hand_over,
        out_shape=tuple(jax.ShapeDtypeStruct(o.shape, o.dtype) for o in out),
        in_specs=[vmem] * 3,
        out_specs=(vmem,) * 3,
        name="hand_over",
    )(*out)


def solution(mesh):
    torus = Mesh(mesh.devices.reshape(NZ, NX, NY, NC), ("z", "x", "y", "c"))
    sp, tp = ("z", "x"), ("y", "c")
    in_specs = (
        P(None, sp, tp),
        P(None, tp),
        P(None, tp),
        P(None, tp),
        P(None, tp),
        P(None, tp),
        P(None, tp),
        P(tp),
        P(tp),
        P(),
        P(None, tp, None),
        P(None, tp, None),
        P(None, tp, None),
        P(None, tp),
        P(None, tp),
    )
    out_specs = (P(None, sp, tp), P(None, tp, sp, None), P(None, tp))
    return jax.shard_map(
        shards, mesh=torus, in_specs=in_specs, out_specs=out_specs, check_vma=False
    )
```

```python
import jax
import jax.numpy as jnp
from jax import lax
from jax.experimental import pallas as pl
from jax.experimental.pallas import tpu as pltpu
from jax.sharding import Mesh
from jax.sharding import PartitionSpec as P

MESH = pl.DeviceIdType.MESH
F32 = jnp.float32
BF = jnp.bfloat16
NZ, NX, NY, NC = 8, 4, 4, 2
L = 192
HALF = L // 2
E = 128
KC = 512
D = 4096
PAD = 16
HE = E // 2
ROWS = E + HE + PAD
PIECES = ((0, 112), (112, 96))


def dot(a, b):
    return jnp.dot(a, b, preferred_element_type=F32)


def dot_nt(a, b):
    return lax.dot_general(a, b, (((1,), (1,)), ((), ())), preferred_element_type=F32)


def dot_tn(a, b):
    return lax.dot_general(a, b, (((0,), (0,)), ((), ())), preferred_element_type=F32)


def split3(x):
    hi = x.astype(BF)
    rest = x - hi.astype(F32)
    mid = rest.astype(BF)
    low = (rest - mid.astype(F32)).astype(BF)
    return hi, mid, low


def compose(later, earlier):
    al, xl = later
    ae, xe = earlier
    grown = jnp.concatenate([ae * xl[:E], xl[E:]], axis=0)
    return al * ae, al * xe + grown - dot(xe.astype(BF), xl[:E].astype(BF))


def apply_map(m, state):
    a, x = m
    return a * state - dot(state.astype(BF), x[:E].astype(BF)) + x[E:]


def tail_rows(a):
    hi, mid, low = split3(a)
    row = lax.broadcasted_iota(jnp.int32, (PAD, E), 0)
    return jnp.where(
        row == 0,
        hi.astype(F32),
        jnp.where(row == 1, mid.astype(F32), jnp.where(row == 2, low.astype(F32), 0.0)),
    ).astype(BF)


def tail_value(rows):
    return jnp.sum(rows.astype(F32), axis=0, keepdims=True)


def kernel(
    bias_ref,
    rate_ref,
    nbeta_ref,
    ndecay_ref,
    tok_ref,
    wq_ref,
    wk_ref,
    wv_ref,
    wg_ref,
    wb_ref,
    wd_ref,
    gain_ref,
    nq_ref,
    nk_ref,
    nv_ref,
    out_ref,
    cache_ref,
    first_ref,
    xbuf,
    wbuf,
    pj,
    acc,
    wbd,
    lo,
    reach,
    sols,
    msg,
    xin,
    zin,
    ret,
    pin,
    side,
    sin,
    wsem,
    tsem,
    ys_sem,
    yr_sem,
    fs_sem,
    fr_sem,
    ps_sem,
    pr_sem,
    xs_sem,
    xr_sem,
    zs_sem,
    zr_sem,
    rs_sem,
    rr_sem,
    ss_sem,
    sr_sem,
):
    z, x, y, c = (lax.axis_index(n) for n in ("z", "x", "y", "c"))
    yu, yd = lax.rem(y + 1, NY), lax.rem(y + NY - 1, NY)
    yf = lax.rem(y + 2, NY)
    head, side_half = x // 2, lax.rem(x, 2)
    other = 1 - c

    def z_at(d):
        return lax.rem(z + d + NZ, NZ)

    def cols(yy, cc):
        return pl.ds(pl.multiple_of((yy * NC + cc) * KC, KC), KC)

    wcopies = []
    for i, w in enumerate((wq_ref, wk_ref, wv_ref, wg_ref)):
        cp = pltpu.make_async_copy(w, wbuf.at[i], wsem.at[i])
        wcopies.append(cp)
    tcopies = []
    for s in range(2):
        cp = pltpu.make_async_copy(tok_ref.at[s], xbuf.at[s, :, cols(y, c)], tsem.at[s])
        cp.start()
        tcopies.append(cp)
    for cp in wcopies:
        cp.start()

    wbd[...] = jnp.concatenate(
        [wb_ref[...].astype(F32), wd_ref[...].astype(F32), jnp.zeros((PAD - 4, D), F32)], axis=0
    ).astype(BF)

    barrier = pltpu.get_barrier_semaphore()
    partners = [{"y": yu}, {"y": yd}, {"c": other}]
    partners += [{"z": z_at(d)} for d in (1, -1, 2, -2)]
    partners += [{"x": lax.rem(x + d, NX)} for d in (1, 2, 3)]
    for p in partners:
        pl.semaphore_signal(barrier, inc=1, device_id=p, device_id_type=MESH)
    pl.semaphore_wait(barrier, len(partners))

    def ycopy(s, half, direction):
        part = xbuf.at[s, pl.ds(half * HALF, HALF), cols(y, c)]
        return pltpu.make_async_remote_copy(
            src_ref=part,
            dst_ref=part,
            send_sem=ys_sem.at[s, half, direction],
            recv_sem=yr_sem.at[s, half, direction],
            device_id={"y": yu if direction == 0 else yd},
            device_id_type=MESH,
        )

    def yarrive(s, half, direction):
        part = xbuf.at[s, pl.ds(half * HALF, HALF), cols(yd if direction == 0 else yu, c)]
        return pltpu.make_async_remote_copy(
            src_ref=part,
            dst_ref=part,
            send_sem=ys_sem.at[s, half, direction],
            recv_sem=yr_sem.at[s, half, direction],
            device_id={"y": yu if direction == 0 else yd},
            device_id_type=MESH,
        )

    def fcopy(s, direction):
        part = xbuf.at[s, pl.ds(direction * HALF, HALF), cols(yd if direction == 0 else yu, c)]
        return pltpu.make_async_remote_copy(
            src_ref=part,
            dst_ref=part,
            send_sem=fs_sem.at[s, direction],
            recv_sem=fr_sem.at[s, direction],
            device_id={"y": yu if direction == 0 else yd},
            device_id_type=MESH,
        )

    def farrive(s, direction):
        part = xbuf.at[s, pl.ds(direction * HALF, HALF), cols(yf, c)]
        return pltpu.make_async_remote_copy(
            src_ref=part,
            dst_ref=part,
            send_sem=fs_sem.at[s, direction],
            recv_sem=fr_sem.at[s, direction],
            device_id={"y": yu if direction == 0 else yd},
            device_id_type=MESH,
        )

    def pcopy(s, k, cc):
        part = xbuf.at[s, :, cols((y, yd, yu, yf)[k], cc)]
        return pltpu.make_async_remote_copy(
            src_ref=part,
            dst_ref=part,
            send_sem=ps_sem.at[s, k],
            recv_sem=pr_sem.at[s, k],
            device_id={"c": other},
            device_id_type=MESH,
        )

    def send_own(s):
        tcopies[s].wait()
        ycopy(s, 0, 0).start()
        ycopy(s, 1, 1).start()
        ycopy(s, 1, 0).start()
        ycopy(s, 0, 1).start()
        pcopy(s, 0, c).start()

    def forward(s):
        yarrive(s, 0, 0).wait_recv()
        fcopy(s, 0).start()
        yarrive(s, 1, 1).wait_recv()
        fcopy(s, 1).start()

    def finish_near(s):
        yarrive(s, 1, 0).wait_recv()
        pcopy(s, 1, c).start()
        yarrive(s, 0, 1).wait_recv()
        pcopy(s, 2, c).start()
        for k in range(3):
            pcopy(s, k, other).wait_recv()

    def finish_far(s):
        farrive(s, 0).wait_recv()
        farrive(s, 1).wait_recv()
        pcopy(s, 3, c).start()
        pcopy(s, 3, other).wait_recv()

    it = lax.broadcasted_iota(jnp.int32, (L, L), 0)
    js = lax.broadcasted_iota(jnp.int32, (L, L), 1)
    lower = it >= js
    strict = it > js

    def project(s, which):
        for i in which:
            pj[s, i] = dot(xbuf[s], wbuf[i]).astype(BF)

    def small(s):
        return dot_nt(xbuf[s], wbd[...])

    def chip(yy):
        return pl.ds(pl.multiple_of(yy * NC * KC, NC * KC), NC * KC)

    def near(s):
        for n, i in enumerate((1, 2)):
            acc[n] = sum(dot(xbuf[s, :, chip(q)], wbuf[i, chip(q), :]) for q in (y, yd, yu))
        return sum(dot_nt(xbuf[s, :, chip(q)], wbd[:, chip(q)]) for q in (y, yd, yu))

    def far(s, part):
        for n, i in enumerate((1, 2)):
            pj[s, i] = (acc[n] + dot(xbuf[s, :, chip(yf)], wbuf[i, chip(yf), :])).astype(BF)
        return part + dot_nt(xbuf[s, :, chip(yf)], wbd[:, chip(yf)])

    heads = range(2)

    def scale(v):
        v = v.astype(F32)
        return lax.rsqrt(jnp.sum(v * v, axis=1, keepdims=True) + 1.0)

    def head_of(s, i, h):
        return pj[s, i, :, h * E : (h + 1) * E]

    def chain_terms(s, bd):
        lane = lax.broadcasted_iota(jnp.int32, (L, PAD), 1)
        bias = jnp.where(lane == 0, bias_ref[0], jnp.where(lane == 1, bias_ref[1], 0.0))
        rate = jnp.where(lane == 2, rate_ref[0], jnp.where(lane == 3, rate_ref[1], 0.0))
        beta = jax.nn.sigmoid(bd + bias)
        soft = jnp.maximum(bd, 0.0) + jnp.log1p(jnp.exp(-jnp.abs(bd)))
        g = -jnp.exp(rate) * soft
        tri = jnp.where(lower, 1.0, 0.0).astype(BF)
        cum = sum(dot(tri, part) for part in split3(g))
        ks = [head_of(s, 1, h) for h in heads]
        vs = [head_of(s, 2, h) for h in heads]
        rk = [scale(v) for v in ks]
        pack = jnp.where(lane == 0, rk[0], jnp.where(lane == 1, rk[1], cum))
        eye = jnp.where(
            lax.broadcasted_iota(jnp.int32, (PAD, PAD), 0)
            == lax.broadcasted_iota(jnp.int32, (PAD, PAD), 1),
            1.0,
            0.0,
        ).astype(BF)
        rows = sum(dot_nt(eye, part) for part in split3(pack))
        amats, cumc, betac = [], [], []
        for h in heads:
            cc = cum[:, 2 + h : 3 + h]
            bc = beta[:, h : h + 1]
            cumc.append(cc)
            betac.append(bc)
            rrow = rows[h : h + 1, :]
            crow = rows[2 + h : 3 + h, :]
            decay = jnp.exp(jnp.where(lower, cc - crow, 0.0)) * rrow
            kk = dot_nt(ks[h], ks[h])
            amats.append(jnp.where(strict, kk * (bc * rk[h]) * decay, 0.0))

        def level_mask(bit):
            return ((it >> (bit + 1)) == (js >> (bit + 1))) & ((it >> bit) != (js >> bit))

        m0 = level_mask(0)
        invs = [-jnp.where(m0, a, 0.0) for a in amats]
        for bit in range(1, 8):
            m = level_mask(bit)
            for h in heads:
                off = jnp.where(m, amats[h], 0.0)
                inv = invs[h]
                ib = inv.astype(BF)
                yy = off + dot(off.astype(BF), ib)
                invs[h] = inv - yy - dot(ib, yy.astype(BF))
        for h in heads:
            b = 2 * s + h
            kf = ks[h].astype(F32)
            ecum = jnp.exp(cumc[h])
            rhs = jnp.concatenate(
                [kf * (betac[h] * rk[h] * ecum), vs[h].astype(F32) * betac[h]], axis=1
            )
            sol = rhs + dot(invs[h].astype(BF), rhs.astype(BF))
            sb = sol.astype(BF)
            last = cumc[h][L - 1 : L, :]
            kd = kf * (rk[h] * jnp.exp(last - cumc[h]))
            rs = dot_tn(sb, kd.astype(BF)).astype(BF)
            msg[s, h, 0:HE, :] = rs[E : E + HE]
            msg[s, h, HE : HE + E, :] = rs[:E]
            msg[s, h, HE + E : ROWS, :] = tail_rows(jnp.broadcast_to(jnp.exp(last), (1, E)))
            msg[s, h, ROWS:, :] = rs[E + HE :]
            sols[b] = sb
        return cumc, rows

    def out_terms(s, cumc, rows):
        for h in heads:
            b = 2 * s + h
            q, k = head_of(s, 0, h), head_of(s, 1, h)
            rq = scale(q)
            cc = cumc[h]
            decay = jnp.exp(jnp.where(lower, cc - rows[2 + h : 3 + h, :], 0.0)) * rows[h : h + 1, :]
            score = jnp.where(lower, dot_nt(q, k) * rq * decay, 0.0).astype(BF)
            sx = dot(score, sols[b])
            lo[b] = sx[:, E:]
            qd = q.astype(F32) * (rq * jnp.exp(cc))
            reach[b] = (qd - sx[:, :E]).astype(BF)

    def xpart(s, t):
        return msg.at[s, t // 2, pl.ds(HE * (t % 2), ROWS)]

    def xcopy(s, t, src_x):
        return pltpu.make_async_remote_copy(
            src_ref=xpart(s, t),
            dst_ref=xin.at[s, src_x],
            send_sem=xs_sem.at[s, t],
            recv_sem=xr_sem.at[s, src_x],
            device_id={"x": t},
            device_id_type=MESH,
        )

    def xlocal(s, t):
        return pltpu.make_async_copy(xpart(s, t), xin.at[s, t], xs_sem.at[s, t])

    def spread(remote, local):
        for t in range(NX):

            @pl.when(x != t)
            def _():
                remote(t).start()

            @pl.when(x == t)
            def _():
                local(t).start()

    def collect(remote, local):
        for t in range(NX):

            @pl.when(x != t)
            def _():
                remote(t).wait_recv()

            @pl.when(x == t)
            def _():
                local(t).wait()

    def xsend(s):
        spread(lambda t: xcopy(s, t, x), lambda t: xlocal(s, t))

    def zcopy(s, slot, piece, hop, dist):
        first, count = PIECES[piece]
        part = zin.at[s, slot, pl.ds(first, count)]
        return pltpu.make_async_remote_copy(
            src_ref=part,
            dst_ref=part,
            send_sem=zs_sem.at[s, dist % NZ, piece],
            recv_sem=zr_sem.at[s, dist % NZ, piece],
            device_id={"z": z_at(hop)},
            device_id_type=MESH,
        )

    def zsend(s):
        collect(lambda t: xcopy(s, t, t), lambda t: xlocal(s, t))
        maps = []
        for j in range(NX):
            r = xin[s, j, pl.ds(pl.multiple_of(HE * (1 - side_half), PAD), E), :]
            a = xin[s, j, pl.ds(pl.multiple_of(E + HE - HE * side_half, PAD), PAD), :]
            v = xin[s, j, pl.ds(pl.multiple_of((E + PAD) * side_half, PAD), HE), :]
            maps.append((tail_value(a), jnp.concatenate([r, v], axis=0).astype(F32)))
        m10 = compose(maps[1], maps[0])
        m32 = compose(maps[3], maps[2])
        a, total = compose(m32, m10)
        zin[s, z, 0 : E + HE, :] = total.astype(BF)
        zin[s, z, E + HE : ROWS, :] = tail_rows(a)
        for hop in (2, -2, 1, -1):
            for piece in range(2):
                zcopy(s, z, piece, hop, hop).start()
        return maps[0], m10, maps[2]

    def zrelay(s):
        for piece in range(2):
            for d in (1, -1):
                slot = z_at(-2 * d)
                zcopy(s, slot, piece, 1, 2 * d).wait_recv()
                zcopy(s, slot, piece, d, 3 * d).start()
                if (piece == 0) == (d == 1):
                    zcopy(s, slot, piece, 2 * d, 4).start()

    def zwait(s, *dists):
        for d in dists:
            for piece in range(2):
                zcopy(s, z_at(-d), piece, 1, d).wait_recv()

    def zmap(s, slot):
        return tail_value(zin[s, slot, E + HE : ROWS, :]), zin[s, slot, 0 : E + HE, :].astype(F32)

    def zmap_if(s, d):
        valid = z + d >= NZ if d > 0 else z + d >= 0
        a, m = zmap(s, z_at(d))
        return jnp.where(valid, a, 1.0), jnp.where(valid, m, 0.0)

    def rcopy(s, t, src_x):
        return pltpu.make_async_remote_copy(
            src_ref=ret.at[s, t],
            dst_ref=pin.at[s, src_x],
            send_sem=rs_sem.at[s, t],
            recv_sem=rr_sem.at[s, src_x],
            device_id={"x": t},
            device_id_type=MESH,
        )

    def rlocal(s, t):
        return pltpu.make_async_copy(ret.at[s, t], pin.at[s, t], rs_sem.at[s, t])

    def scopy(s, t, src_x):
        return pltpu.make_async_remote_copy(
            src_ref=side.at[s, t],
            dst_ref=sin.at[s, src_x],
            send_sem=ss_sem.at[s, t],
            recv_sem=sr_sem.at[s, src_x],
            device_id={"x": t},
            device_id_type=MESH,
        )

    def slocal(s, t):
        return pltpu.make_async_copy(side.at[s, t], sin.at[s, t], ss_sem.at[s, t])

    def start_states(s, inner):
        zwait(s, 1, -1)
        behind = compose(zmap_if(s, -1), zmap_if(s, -2))
        early = apply_map(zmap_if(s, 2), zmap_if(s, 1)[1][E:])
        zwait(s, 3, -3, 4)
        behind = compose(behind, zmap_if(s, -3))
        early = apply_map(zmap_if(s, -4), apply_map(zmap_if(s, 3), early))
        here = apply_map(behind, early)
        m0, m10, m2 = inner
        second = apply_map(m10, here)
        ret[s, 0] = here.astype(BF)
        ret[s, 1] = apply_map(m0, here).astype(BF)
        ret[s, 2] = second.astype(BF)
        ret[s, 3] = apply_map(m2, second).astype(BF)
        spread(lambda t: rcopy(s, t, x), lambda t: rlocal(s, t))

    def unit(v):
        return v * lax.rsqrt(jnp.sum(v * v, axis=1, keepdims=True) + 1.0)

    gain = gain_ref[...]

    def final_parts(s):
        state = apply_map(zmap(s, 1), zmap(s, 0)[1][E:])
        for k in (2, 4, 6):
            state = apply_map(compose(zmap(s, k + 1), zmap(s, k)), state)
        place = lax.broadcasted_iota(jnp.int32, (HE, E), 1) == (
            lax.broadcasted_iota(jnp.int32, (HE, E), 0) + HE * side_half
        )
        memf = dot_tn(state.astype(BF), jnp.where(place, 1.0, 0.0).astype(BF))
        memory = memf.astype(BF)

        def pick(ref):
            row = ref[s].astype(F32)
            return jnp.where(head == 0, row[0:1, :], row[1:2, :])

        qn, kn, nv = unit(pick(nq_ref)), unit(pick(nk_ref)), pick(nv_ref)
        nbeta = jnp.where(head == 0, nbeta_ref[s, 0], nbeta_ref[s, 1])
        ndecay = jnp.where(head == 0, ndecay_ref[s, 0], ndecay_ref[s, 1])
        row = lax.broadcasted_iota(jnp.int32, (PAD, E), 0)
        asked = jnp.where(row == 0, qn, jnp.where(row == 1, kn, 0.0))
        seen = sum(dot(part, memory) for part in split3(asked))
        recall, retrieve = seen[0:1, :], seen[1:2, :]
        intersect = jnp.sum(kn * qn, axis=1, keepdims=True)
        lane = lax.broadcasted_iota(jnp.int32, (1, E), 1)
        nv = jnp.where((lane >= HE) == (side_half == 1), nv, 0.0)
        fresh = nv - ndecay * retrieve
        read = ndecay * recall + (nbeta * intersect) * fresh
        mine = memf[0:16, :]
        for k in range(1, NZ):
            mine = jnp.where(z == k, memf[16 * k : 16 * k + 16, :], mine)
        for t in range(NX):
            side[s, t, 0:4, :] = mine[4 * t : 4 * t + 4, :]
            side[s, t, 4:8, :] = jnp.broadcast_to(read, (4, E))
        spread(lambda t: scopy(s, t, x), lambda t: slocal(s, t))

    def outputs(s):
        collect(lambda t: rcopy(s, t, t), lambda t: rlocal(s, t))
        for h in heads:
            b = 2 * s + h
            start = jnp.concatenate([pin[s, 2 * h], pin[s, 2 * h + 1]], axis=0)
            o = lo[b] + dot_nt(reach[b], start)
            gate = head_of(s, 3, h).astype(F32)
            norm = lax.rsqrt(jnp.mean(o * o, axis=1, keepdims=True) + 0.001)
            out_ref[s, :, h * E : (h + 1) * E] = (
                o * norm * gain * (gate * jax.nn.sigmoid(gate))
            ).astype(BF)

    def last_parts(s):
        collect(lambda t: scopy(s, t, t), lambda t: slocal(s, t))
        for h in heads:
            both = sin[s, 2 * h] + sin[s, 2 * h + 1]
            cache_ref[s, h] = both[0:4].astype(BF)
            read = both[4:5]
            norm = lax.rsqrt(jnp.mean(read * read, axis=1, keepdims=True) + 0.001)
            first_ref[s : s + 1, h * E : (h + 1) * E] = read * norm * gain

    send_own(0)
    forward(0)
    send_own(1)
    finish_near(0)
    finish_far(0)
    for cp in wcopies:
        cp.wait()
    project(0, (1, 2))
    forward(1)
    kept0 = chain_terms(0, small(0))
    xsend(0)
    project(0, (0, 3))
    out_terms(0, *kept0)
    finish_near(1)
    part = near(1)
    inner0 = zsend(0)
    finish_far(1)
    kept1 = chain_terms(1, far(1, part))
    xsend(1)
    zrelay(0)
    project(1, (0, 3))
    out_terms(1, *kept1)
    inner1 = zsend(1)
    start_states(0, inner0)
    zrelay(1)
    final_parts(0)
    outputs(0)
    start_states(1, inner1)
    final_parts(1)
    last_parts(0)
    outputs(1)
    last_parts(1)

    for s in range(2):
        for half in range(2):
            for direction in range(2):
                ycopy(s, half, direction).wait_send()
        for direction in range(2):
            fcopy(s, direction).wait_send()
        for k in range(4):
            pcopy(s, k, c).wait_send()
        for t in range(NX):

            @pl.when(x != t)
            def _():
                xcopy(s, t, x).wait_send()
                rcopy(s, t, x).wait_send()
                scopy(s, t, x).wait_send()

        for hop in (2, -2, 1, -1):
            for piece in range(2):
                zcopy(s, z, piece, hop, hop).wait_send()
        for piece in range(2):
            for d in (1, -1):
                zcopy(s, z_at(-2 * d), piece, d, 3 * d).wait_send()
                if (piece == 0) == (d == 1):
                    zcopy(s, z_at(-2 * d), piece, 2 * d, 4).wait_send()


def hand_over(mixed_in, cache_in, first_in, mixed_out, cache_out, first_out):
    mixed_out[...] = mixed_in[...]
    cache_out[...] = cache_in[...]
    first_out[...] = first_in[...]


def shards(
    tokens,
    query_weight,
    key_weight,
    value_weight,
    gate_weight,
    beta_weight,
    decay_weight,
    beta_bias,
    rate_log,
    out_gain,
    new_query,
    new_key,
    new_value,
    new_beta,
    new_decay,
):
    smem = pl.BlockSpec(memory_space=pltpu.SMEM)
    vmem = pl.BlockSpec(memory_space=pltpu.VMEM)
    hbm = pl.BlockSpec(memory_space=pl.ANY)
    dma = pltpu.SemaphoreType.DMA
    out = pl.pallas_call(
        kernel,
        out_shape=(
            jax.ShapeDtypeStruct((2, L, 2 * E), BF),
            jax.ShapeDtypeStruct((2, 2, 4, E), BF),
            jax.ShapeDtypeStruct((2, 2 * E), F32),
        ),
        in_specs=[smem] * 4 + [hbm] * 5 + [vmem] * 6,
        out_specs=(vmem, vmem, vmem),
        scratch_shapes=[
            pltpu.VMEM((2, L, D), BF),
            pltpu.VMEM((4, D, 2 * E), BF),
            pltpu.VMEM((2, 4, L, 2 * E), BF),
            pltpu.VMEM((2, L, 2 * E), F32),
            pltpu.VMEM((PAD, D), BF),
            pltpu.VMEM((4, L, E), F32),
            pltpu.VMEM((4, L, E), BF),
            pltpu.VMEM((4, L, 2 * E), BF),
            pltpu.VMEM((2, 2, E + 2 * HE + PAD, E), BF),
            pltpu.VMEM((2, NX, ROWS, E), BF),
            pltpu.VMEM((2, NZ, ROWS, E), BF),
            pltpu.VMEM((2, NX, HE, E), BF),
            pltpu.VMEM((2, NX, HE, E), BF),
            pltpu.VMEM((2, NX, 8, E), F32),
            pltpu.VMEM((2, NX, 8, E), F32),
            dma((4,)),
            dma((2,)),
            dma((2, 2, 2)),
            dma((2, 2, 2)),
            dma((2, 2)),
            dma((2, 2)),
            dma((2, 4)),
            dma((2, 4)),
            dma((2, NX)),
            dma((2, NX)),
            dma((2, NZ, 2)),
            dma((2, NZ, 2)),
            dma((2, NX)),
            dma((2, NX)),
            dma((2, NX)),
            dma((2, NX)),
        ],
        compiler_params=pltpu.CompilerParams(
            collective_id=0, has_side_effects=True, vmem_limit_bytes=60 * 1024 * 1024
        ),
        name="delta_all",
    )(
        beta_bias,
        rate_log,
        new_beta,
        new_decay,
        tokens,
        query_weight,
        key_weight,
        value_weight,
        gate_weight,
        beta_weight.T,
        decay_weight.T,
        out_gain.reshape(1, E),
        new_query,
        new_key,
        new_value,
    )
    return pl.pallas_call(
        hand_over,
        out_shape=tuple(jax.ShapeDtypeStruct(o.shape, o.dtype) for o in out),
        in_specs=[vmem] * 3,
        out_specs=(vmem,) * 3,
        name="hand_over",
    )(*out)


def solution(mesh):
    torus = Mesh(mesh.devices.reshape(NZ, NX, NY, NC), ("z", "x", "y", "c"))
    sp, tp = ("z", "x"), ("y", "c")
    in_specs = (
        P(None, sp, tp),
        P(None, tp),
        P(None, tp),
        P(None, tp),
        P(None, tp),
        P(None, tp),
        P(None, tp),
        P(tp),
        P(tp),
        P(),
        P(None, tp, None),
        P(None, tp, None),
        P(None, tp, None),
        P(None, tp),
        P(None, tp),
    )
    out_specs = (P(None, sp, tp), P(None, tp, sp, None), P(None, tp))
    return jax.shard_map(
        shards, mesh=torus, in_specs=in_specs, out_specs=out_specs, check_vma=False
    )
```

```python
import jax
import jax.numpy as jnp
from jax import lax
from jax.experimental import pallas as pl
from jax.experimental.pallas import tpu as pltpu
from jax.sharding import Mesh
from jax.sharding import PartitionSpec as P

MESH = pl.DeviceIdType.MESH
F32 = jnp.float32
BF = jnp.bfloat16
NZ, NX, NY, NC = 8, 4, 4, 2
L = 192
HALF = L // 2
E = 128
KC = 512
D = 4096
PAD = 16
BLOCK = 64
HE = E // 2
ROWS = E + HE + PAD
PIECES = ((0, 112), (112, 96))


def dot(a, b):
    return jnp.dot(a, b, preferred_element_type=F32)


def dot_nt(a, b):
    return lax.dot_general(a, b, (((1,), (1,)), ((), ())), preferred_element_type=F32)


def dot_tn(a, b):
    return lax.dot_general(a, b, (((0,), (0,)), ((), ())), preferred_element_type=F32)


def split3(x):
    hi = x.astype(BF)
    rest = x - hi.astype(F32)
    mid = rest.astype(BF)
    low = (rest - mid.astype(F32)).astype(BF)
    return hi, mid, low


def compose(later, earlier):
    al, xl = later
    ae, xe = earlier
    grown = jnp.concatenate([ae * xl[:E], xl[E:]], axis=0)
    return al * ae, al * xe + grown - dot(xe.astype(BF), xl[:E].astype(BF))


def apply_map(m, state):
    a, x = m
    return a * state - dot(state.astype(BF), x[:E].astype(BF)) + x[E:]


def tail_rows(a):
    hi, mid, low = split3(a)
    row = lax.broadcasted_iota(jnp.int32, (PAD, E), 0)
    return jnp.where(
        row == 0,
        hi.astype(F32),
        jnp.where(row == 1, mid.astype(F32), jnp.where(row == 2, low.astype(F32), 0.0)),
    ).astype(BF)


def tail_value(rows):
    return jnp.sum(rows.astype(F32), axis=0, keepdims=True)


def kernel(
    bias_ref,
    rate_ref,
    nbeta_ref,
    ndecay_ref,
    tok_ref,
    wq_ref,
    wk_ref,
    wv_ref,
    wg_ref,
    wb_ref,
    wd_ref,
    gain_ref,
    nq_ref,
    nk_ref,
    nv_ref,
    out_ref,
    cache_ref,
    first_ref,
    xbuf,
    wbuf,
    pj,
    acc,
    wbd,
    lo,
    reach,
    sols,
    msg,
    xin,
    zin,
    ret,
    pin,
    side,
    sin,
    wsem,
    tsem,
    ys_sem,
    yr_sem,
    fs_sem,
    fr_sem,
    ps_sem,
    pr_sem,
    xs_sem,
    xr_sem,
    zs_sem,
    zr_sem,
    rs_sem,
    rr_sem,
    ss_sem,
    sr_sem,
):
    z, x, y, c = (lax.axis_index(n) for n in ("z", "x", "y", "c"))
    yu, yd = lax.rem(y + 1, NY), lax.rem(y + NY - 1, NY)
    yf = lax.rem(y + 2, NY)
    head, side_half = x // 2, lax.rem(x, 2)
    other = 1 - c

    def z_at(d):
        return lax.rem(z + d + NZ, NZ)

    def cols(yy, cc):
        return pl.ds(pl.multiple_of((yy * NC + cc) * KC, KC), KC)

    wcopies = []
    for i, w in enumerate((wq_ref, wk_ref, wv_ref, wg_ref)):
        cp = pltpu.make_async_copy(w, wbuf.at[i], wsem.at[i])
        wcopies.append(cp)
    tcopies = []
    for s in range(2):
        cp = pltpu.make_async_copy(tok_ref.at[s], xbuf.at[s, :, cols(y, c)], tsem.at[s])
        cp.start()
        tcopies.append(cp)
    for cp in wcopies:
        cp.start()

    barrier = pltpu.get_barrier_semaphore()
    partners = [{"y": yu}, {"y": yd}, {"c": other}]
    partners += [{"z": z_at(d)} for d in (1, -1, 2, -2)]
    partners += [{"x": lax.rem(x + d, NX)} for d in (1, 2, 3)]
    for p in partners:
        pl.semaphore_signal(barrier, inc=1, device_id=p, device_id_type=MESH)
    small_rows = jnp.concatenate(
        [wb_ref[...].astype(F32), wd_ref[...].astype(F32), jnp.zeros((PAD - 4, D), F32)], axis=0
    )
    wbd[...] = small_rows.T.astype(BF)
    pl.semaphore_wait(barrier, len(partners))

    def ycopy(s, half, direction):
        part = xbuf.at[s, pl.ds(half * HALF, HALF), cols(y, c)]
        return pltpu.make_async_remote_copy(
            src_ref=part,
            dst_ref=part,
            send_sem=ys_sem.at[s, half, direction],
            recv_sem=yr_sem.at[s, half, direction],
            device_id={"y": yu if direction == 0 else yd},
            device_id_type=MESH,
        )

    def yarrive(s, half, direction):
        part = xbuf.at[s, pl.ds(half * HALF, HALF), cols(yd if direction == 0 else yu, c)]
        return pltpu.make_async_remote_copy(
            src_ref=part,
            dst_ref=part,
            send_sem=ys_sem.at[s, half, direction],
            recv_sem=yr_sem.at[s, half, direction],
            device_id={"y": yu if direction == 0 else yd},
            device_id_type=MESH,
        )

    def fcopy(s, direction):
        part = xbuf.at[s, pl.ds(direction * HALF, HALF), cols(yd if direction == 0 else yu, c)]
        return pltpu.make_async_remote_copy(
            src_ref=part,
            dst_ref=part,
            send_sem=fs_sem.at[s, direction],
            recv_sem=fr_sem.at[s, direction],
            device_id={"y": yu if direction == 0 else yd},
            device_id_type=MESH,
        )

    def farrive(s, direction):
        part = xbuf.at[s, pl.ds(direction * HALF, HALF), cols(yf, c)]
        return pltpu.make_async_remote_copy(
            src_ref=part,
            dst_ref=part,
            send_sem=fs_sem.at[s, direction],
            recv_sem=fr_sem.at[s, direction],
            device_id={"y": yu if direction == 0 else yd},
            device_id_type=MESH,
        )

    def pcopy(s, k, cc):
        part = xbuf.at[s, :, cols((y, yd, yu, yf)[k], cc)]
        return pltpu.make_async_remote_copy(
            src_ref=part,
            dst_ref=part,
            send_sem=ps_sem.at[s, k],
            recv_sem=pr_sem.at[s, k],
            device_id={"c": other},
            device_id_type=MESH,
        )

    def send_own(s):
        tcopies[s].wait()
        ycopy(s, 0, 0).start()
        ycopy(s, 1, 1).start()
        ycopy(s, 1, 0).start()
        ycopy(s, 0, 1).start()
        pcopy(s, 0, c).start()

    def forward(s):
        yarrive(s, 0, 0).wait_recv()
        fcopy(s, 0).start()
        yarrive(s, 1, 1).wait_recv()
        fcopy(s, 1).start()

    def near_start(s):
        yarrive(s, 1, 0).wait_recv()
        pcopy(s, 1, c).start()
        yarrive(s, 0, 1).wait_recv()
        pcopy(s, 2, c).start()

    def near_end(s):
        for k in range(3):
            pcopy(s, k, other).wait_recv()

    def far_start(s):
        farrive(s, 0).wait_recv()
        farrive(s, 1).wait_recv()
        pcopy(s, 3, c).start()

    def far_end(s):
        pcopy(s, 3, other).wait_recv()

    it = lax.broadcasted_iota(jnp.int32, (L, L), 0)
    js = lax.broadcasted_iota(jnp.int32, (L, L), 1)
    lower = it >= js
    bt = lax.broadcasted_iota(jnp.int32, (BLOCK, BLOCK), 0)
    bs = lax.broadcasted_iota(jnp.int32, (BLOCK, BLOCK), 1)

    def project(s, which):
        for i in which:
            pj[s, i] = dot(xbuf[s], wbuf[i]).astype(BF)

    def chip(yy):
        return pl.ds(pl.multiple_of(yy * NC * KC, NC * KC), NC * KC)

    def near(s):
        for n, i in enumerate((1, 2)):
            acc[n] = sum(dot(xbuf[s, :, chip(q)], wbuf[i, chip(q), :]) for q in (y, yd, yu))
        return sum(dot(xbuf[s, :, chip(q)], wbd[chip(q), :]) for q in (y, yd, yu))

    def far(s, part):
        for n, i in enumerate((1, 2)):
            pj[s, i] = (acc[n] + dot(xbuf[s, :, chip(yf)], wbuf[i, chip(yf), :])).astype(BF)
        return part + dot(xbuf[s, :, chip(yf)], wbd[chip(yf), :])

    heads = range(2)

    def scale(v):
        v = v.astype(F32)
        return lax.rsqrt(jnp.sum(v * v, axis=1, keepdims=True) + 1.0)

    def head_of(s, i, h):
        return pj[s, i, :, h * E : (h + 1) * E]

    def chain_terms(s, bd, between):
        lane = lax.broadcasted_iota(jnp.int32, (L, PAD), 1)
        bias = jnp.where(lane == 0, bias_ref[0], jnp.where(lane == 1, bias_ref[1], 0.0))
        rate = jnp.where(lane == 2, rate_ref[0], jnp.where(lane == 3, rate_ref[1], 0.0))
        beta = jax.nn.sigmoid(bd + bias)
        soft = jnp.maximum(bd, 0.0) + jnp.log1p(jnp.exp(-jnp.abs(bd)))
        g = -jnp.exp(rate) * soft
        tri = jnp.where(lower, 1.0, 0.0).astype(BF)
        cum = sum(dot(tri, part) for part in split3(g))
        ks = [head_of(s, 1, h) for h in heads]
        vs = [head_of(s, 2, h) for h in heads]
        rk = [scale(v) for v in ks]
        pack = jnp.where(lane == 0, rk[0], jnp.where(lane == 1, rk[1], cum))
        eye = jnp.where(
            lax.broadcasted_iota(jnp.int32, (PAD, PAD), 0)
            == lax.broadcasted_iota(jnp.int32, (PAD, PAD), 1),
            1.0,
            0.0,
        ).astype(BF)
        rows = sum(dot_nt(eye, part) for part in split3(pack))
        cumc = [cum[:, 2 + h : 3 + h] for h in heads]
        betac = [beta[:, h : h + 1] for h in heads]

        def corner(h, top, count, left):
            span = slice(top, top + count)
            kk = dot_nt(ks[h][span], ks[h][left : left + BLOCK])
            gap = cumc[h][span] - rows[2 + h : 3 + h, left : left + BLOCK]
            if top == left:
                gap = jnp.where(bt > bs, gap, 0.0)
            value = kk * (betac[h] * rk[h])[span] * jnp.exp(gap) * rows[h : h + 1, left : left + BLOCK]
            return jnp.where(bt > bs, value, 0.0) if top == left else value

        def level_mask(bit):
            return ((bt >> (bit + 1)) == (bs >> (bit + 1))) & ((bt >> bit) != (bs >> bit))

        diag = [corner(h, BLOCK * n, BLOCK, BLOCK * n) for h in heads for n in range(3)]
        m = level_mask(0)
        invs = [-jnp.where(m, a, 0.0) for a in diag]
        for bit in range(1, 6):
            m = level_mask(bit)
            halfway = []
            for a, inv in zip(diag, invs):
                off = jnp.where(m, a, 0.0)
                halfway.append(off + dot(off.astype(BF), inv.astype(BF)))
            invs = [
                inv - yy - dot(inv.astype(BF), yy.astype(BF)) for inv, yy in zip(invs, halfway)
            ]
        invs = [inv.astype(BF) for inv in invs]
        between()
        rhs, sols_of = [], [[], []]
        for h in heads:
            kf = ks[h].astype(F32)
            rhs.append(
                jnp.concatenate(
                    [
                        kf * (betac[h] * rk[h] * jnp.exp(cumc[h])),
                        vs[h].astype(F32) * betac[h],
                    ],
                    axis=1,
                )
            )
        rest = rhs
        for n in range(3):
            for h in heads:
                now = rest[h][:BLOCK]
                sols_of[h].append((now + dot(invs[3 * h + n], now.astype(BF))).astype(BF))
            if n < 2:
                rest = [
                    rest[h][BLOCK:]
                    - dot(
                        corner(h, BLOCK * (n + 1), L - BLOCK * (n + 1), BLOCK * n).astype(BF),
                        sols_of[h][n],
                    )
                    for h in heads
                ]
        for h in heads:
            b = 2 * s + h
            kf = ks[h].astype(F32)
            sb = jnp.concatenate(sols_of[h], axis=0)
            last = cumc[h][L - 1 : L, :]
            kd = kf * (rk[h] * jnp.exp(last - cumc[h]))
            rs = dot_tn(sb, kd.astype(BF)).astype(BF)
            msg[s, h, 0:HE, :] = rs[E : E + HE]
            msg[s, h, HE : HE + E, :] = rs[:E]
            msg[s, h, HE + E : ROWS, :] = tail_rows(jnp.broadcast_to(jnp.exp(last), (1, E)))
            msg[s, h, ROWS:, :] = rs[E + HE :]
            sols[b] = sb
        return cumc, rows

    def out_terms(s, cumc, rows):
        for h in heads:
            b = 2 * s + h
            q, k = head_of(s, 0, h), head_of(s, 1, h)
            rq = scale(q)
            cc = cumc[h]
            decay = jnp.exp(jnp.where(lower, cc - rows[2 + h : 3 + h, :], 0.0)) * rows[h : h + 1, :]
            score = jnp.where(lower, dot_nt(q, k) * rq * decay, 0.0).astype(BF)
            sx = dot(score, sols[b])
            lo[b] = sx[:, E:]
            qd = q.astype(F32) * (rq * jnp.exp(cc))
            reach[b] = (qd - sx[:, :E]).astype(BF)

    def xpart(s, t):
        return msg.at[s, t // 2, pl.ds(HE * (t % 2), ROWS)]

    def xcopy(s, t, src_x):
        return pltpu.make_async_remote_copy(
            src_ref=xpart(s, t),
            dst_ref=xin.at[s, src_x],
            send_sem=xs_sem.at[s, t],
            recv_sem=xr_sem.at[s, src_x],
            device_id={"x": t},
            device_id_type=MESH,
        )

    def xlocal(s, t):
        return pltpu.make_async_copy(xpart(s, t), xin.at[s, t], xs_sem.at[s, t])

    def spread(remote, local):
        for t in range(NX):

            @pl.when(x != t)
            def _():
                remote(t).start()

            @pl.when(x == t)
            def _():
                local(t).start()

    def collect(remote, local):
        for t in range(NX):

            @pl.when(x != t)
            def _():
                remote(t).wait_recv()

            @pl.when(x == t)
            def _():
                local(t).wait()

    def xsend(s):
        spread(lambda t: xcopy(s, t, x), lambda t: xlocal(s, t))

    def zcopy(s, slot, piece, hop, dist):
        first, count = PIECES[piece]
        part = zin.at[s, slot, pl.ds(first, count)]
        return pltpu.make_async_remote_copy(
            src_ref=part,
            dst_ref=part,
            send_sem=zs_sem.at[s, dist % NZ, piece],
            recv_sem=zr_sem.at[s, dist % NZ, piece],
            device_id={"z": z_at(hop)},
            device_id_type=MESH,
        )

    def zsend(s):
        collect(lambda t: xcopy(s, t, t), lambda t: xlocal(s, t))
        maps = []
        for j in range(NX):
            r = xin[s, j, pl.ds(pl.multiple_of(HE * (1 - side_half), PAD), E), :]
            a = xin[s, j, pl.ds(pl.multiple_of(E + HE - HE * side_half, PAD), PAD), :]
            v = xin[s, j, pl.ds(pl.multiple_of((E + PAD) * side_half, PAD), HE), :]
            maps.append((tail_value(a), jnp.concatenate([r, v], axis=0).astype(F32)))
        m10 = compose(maps[1], maps[0])
        m32 = compose(maps[3], maps[2])
        a, total = compose(m32, m10)
        zin[s, z, 0 : E + HE, :] = total.astype(BF)
        zin[s, z, E + HE : ROWS, :] = tail_rows(a)
        for hop in (2, -2, 1, -1):
            for piece in range(2):
                zcopy(s, z, piece, hop, hop).start()
        return maps[0], m10, maps[2]

    def zrelay(s):
        for piece in range(2):
            for d in (1, -1):
                slot = z_at(-2 * d)
                zcopy(s, slot, piece, 1, 2 * d).wait_recv()
                zcopy(s, slot, piece, d, 3 * d).start()
                if (piece == 0) == (d == 1):
                    zcopy(s, slot, piece, 2 * d, 4).start()

    def zwait(s, *dists):
        for d in dists:
            for piece in range(2):
                zcopy(s, z_at(-d), piece, 1, d).wait_recv()

    def zmap(s, slot):
        return tail_value(zin[s, slot, E + HE : ROWS, :]), zin[s, slot, 0 : E + HE, :].astype(F32)

    def zmap_if(s, d):
        valid = z + d >= NZ if d > 0 else z + d >= 0
        a, m = zmap(s, z_at(d))
        return jnp.where(valid, a, 1.0), jnp.where(valid, m, 0.0)

    def rcopy(s, t, src_x):
        return pltpu.make_async_remote_copy(
            src_ref=ret.at[s, t],
            dst_ref=pin.at[s, src_x],
            send_sem=rs_sem.at[s, t],
            recv_sem=rr_sem.at[s, src_x],
            device_id={"x": t},
            device_id_type=MESH,
        )

    def rlocal(s, t):
        return pltpu.make_async_copy(ret.at[s, t], pin.at[s, t], rs_sem.at[s, t])

    def scopy(s, t, src_x):
        return pltpu.make_async_remote_copy(
            src_ref=side.at[s, t],
            dst_ref=sin.at[s, src_x],
            send_sem=ss_sem.at[s, t],
            recv_sem=sr_sem.at[s, src_x],
            device_id={"x": t},
            device_id_type=MESH,
        )

    def slocal(s, t):
        return pltpu.make_async_copy(side.at[s, t], sin.at[s, t], ss_sem.at[s, t])

    def start_states(s, inner):
        zwait(s, 1, -1)
        behind = compose(zmap_if(s, -1), zmap_if(s, -2))
        early = apply_map(zmap_if(s, 2), zmap_if(s, 1)[1][E:])
        zwait(s, 3, -3, 4)
        behind = compose(behind, zmap_if(s, -3))
        early = apply_map(zmap_if(s, -4), apply_map(zmap_if(s, 3), early))
        here = apply_map(behind, early)
        m0, m10, m2 = inner
        second = apply_map(m10, here)
        ret[s, 0] = here.astype(BF)
        ret[s, 1] = apply_map(m0, here).astype(BF)
        ret[s, 2] = second.astype(BF)
        ret[s, 3] = apply_map(m2, second).astype(BF)
        spread(lambda t: rcopy(s, t, x), lambda t: rlocal(s, t))

    def unit(v):
        return v * lax.rsqrt(jnp.sum(v * v, axis=1, keepdims=True) + 1.0)

    gain = gain_ref[...]

    def final_parts(s):
        state = apply_map(zmap(s, 1), zmap(s, 0)[1][E:])
        for k in (2, 4, 6):
            state = apply_map(compose(zmap(s, k + 1), zmap(s, k)), state)
        place = lax.broadcasted_iota(jnp.int32, (HE, E), 1) == (
            lax.broadcasted_iota(jnp.int32, (HE, E), 0) + HE * side_half
        )
        memf = dot_tn(state.astype(BF), jnp.where(place, 1.0, 0.0).astype(BF))
        memory = memf.astype(BF)

        def pick(ref):
            row = ref[s].astype(F32)
            return jnp.where(head == 0, row[0:1, :], row[1:2, :])

        qn, kn, nv = unit(pick(nq_ref)), unit(pick(nk_ref)), pick(nv_ref)
        nbeta = jnp.where(head == 0, nbeta_ref[s, 0], nbeta_ref[s, 1])
        ndecay = jnp.where(head == 0, ndecay_ref[s, 0], ndecay_ref[s, 1])
        row = lax.broadcasted_iota(jnp.int32, (PAD, E), 0)
        asked = jnp.where(row == 0, qn, jnp.where(row == 1, kn, 0.0))
        seen = sum(dot(part, memory) for part in split3(asked))
        recall, retrieve = seen[0:1, :], seen[1:2, :]
        intersect = jnp.sum(kn * qn, axis=1, keepdims=True)
        lane = lax.broadcasted_iota(jnp.int32, (1, E), 1)
        nv = jnp.where((lane >= HE) == (side_half == 1), nv, 0.0)
        fresh = nv - ndecay * retrieve
        read = ndecay * recall + (nbeta * intersect) * fresh
        mine = memf[0:16, :]
        for k in range(1, NZ):
            mine = jnp.where(z == k, memf[16 * k : 16 * k + 16, :], mine)
        for t in range(NX):
            side[s, t, 0:4, :] = mine[4 * t : 4 * t + 4, :]
            side[s, t, 4:8, :] = jnp.broadcast_to(read, (4, E))
        spread(lambda t: scopy(s, t, x), lambda t: slocal(s, t))

    def outputs(s):
        collect(lambda t: rcopy(s, t, t), lambda t: rlocal(s, t))
        for h in heads:
            b = 2 * s + h
            start = jnp.concatenate([pin[s, 2 * h], pin[s, 2 * h + 1]], axis=0)
            o = lo[b] + dot_nt(reach[b], start)
            gate = head_of(s, 3, h).astype(F32)
            norm = lax.rsqrt(jnp.mean(o * o, axis=1, keepdims=True) + 0.001)
            out_ref[s, :, h * E : (h + 1) * E] = (
                o * norm * gain * (gate * jax.nn.sigmoid(gate))
            ).astype(BF)

    def last_parts(s):
        collect(lambda t: scopy(s, t, t), lambda t: slocal(s, t))
        for h in heads:
            both = sin[s, 2 * h] + sin[s, 2 * h + 1]
            cache_ref[s, h] = both[0:4].astype(BF)
            read = both[4:5]
            norm = lax.rsqrt(jnp.mean(read * read, axis=1, keepdims=True) + 0.001)
            first_ref[s : s + 1, h * E : (h + 1) * E] = read * norm * gain

    inner = []
    send_own(0)
    forward(0)
    send_own(1)
    near_start(0)
    near_end(0)
    far_start(0)
    for cp in wcopies:
        cp.wait()
    part = near(0)
    forward(1)
    far_end(0)
    kept0 = chain_terms(0, far(0, part), lambda: near_start(1))
    xsend(0)
    far_start(1)
    near_end(1)
    part = near(1)
    far_end(1)
    kept1 = chain_terms(1, far(1, part), lambda: inner.append(zsend(0)))
    xsend(1)
    project(0, (0, 3))
    out_terms(0, *kept0)
    project(1, (0, 3))
    zrelay(0)
    out_terms(1, *kept1)
    inner.append(zsend(1))
    zrelay(1)
    start_states(0, inner[0])
    final_parts(0)
    start_states(1, inner[1])
    final_parts(1)
    outputs(0)
    last_parts(0)
    outputs(1)
    last_parts(1)

    for s in range(2):
        for half in range(2):
            for direction in range(2):
                ycopy(s, half, direction).wait_send()
        for direction in range(2):
            fcopy(s, direction).wait_send()
        for k in range(4):
            pcopy(s, k, c).wait_send()
        for t in range(NX):

            @pl.when(x != t)
            def _():
                xcopy(s, t, x).wait_send()
                rcopy(s, t, x).wait_send()
                scopy(s, t, x).wait_send()

        for hop in (2, -2, 1, -1):
            for piece in range(2):
                zcopy(s, z, piece, hop, hop).wait_send()
        for piece in range(2):
            for d in (1, -1):
                zcopy(s, z_at(-2 * d), piece, d, 3 * d).wait_send()
                if (piece == 0) == (d == 1):
                    zcopy(s, z_at(-2 * d), piece, 2 * d, 4).wait_send()


def hand_over(mixed_in, cache_in, first_in, mixed_out, cache_out, first_out):
    mixed_out[...] = mixed_in[...]
    cache_out[...] = cache_in[...]
    first_out[...] = first_in[...]


def shards(
    tokens,
    query_weight,
    key_weight,
    value_weight,
    gate_weight,
    beta_weight,
    decay_weight,
    beta_bias,
    rate_log,
    out_gain,
    new_query,
    new_key,
    new_value,
    new_beta,
    new_decay,
):
    smem = pl.BlockSpec(memory_space=pltpu.SMEM)
    vmem = pl.BlockSpec(memory_space=pltpu.VMEM)
    hbm = pl.BlockSpec(memory_space=pl.ANY)
    dma = pltpu.SemaphoreType.DMA
    out = pl.pallas_call(
        kernel,
        out_shape=(
            jax.ShapeDtypeStruct((2, L, 2 * E), BF),
            jax.ShapeDtypeStruct((2, 2, 4, E), BF),
            jax.ShapeDtypeStruct((2, 2 * E), F32),
        ),
        in_specs=[smem] * 4 + [hbm] * 5 + [vmem] * 6,
        out_specs=(vmem, vmem, vmem),
        scratch_shapes=[
            pltpu.VMEM((2, L, D), BF),
            pltpu.VMEM((4, D, 2 * E), BF),
            pltpu.VMEM((2, 4, L, 2 * E), BF),
            pltpu.VMEM((2, L, 2 * E), F32),
            pltpu.VMEM((D, PAD), BF),
            pltpu.VMEM((4, L, E), F32),
            pltpu.VMEM((4, L, E), BF),
            pltpu.VMEM((4, L, 2 * E), BF),
            pltpu.VMEM((2, 2, E + 2 * HE + PAD, E), BF),
            pltpu.VMEM((2, NX, ROWS, E), BF),
            pltpu.VMEM((2, NZ, ROWS, E), BF),
            pltpu.VMEM((2, NX, HE, E), BF),
            pltpu.VMEM((2, NX, HE, E), BF),
            pltpu.VMEM((2, NX, 8, E), F32),
            pltpu.VMEM((2, NX, 8, E), F32),
            dma((4,)),
            dma((2,)),
            dma((2, 2, 2)),
            dma((2, 2, 2)),
            dma((2, 2)),
            dma((2, 2)),
            dma((2, 4)),
            dma((2, 4)),
            dma((2, NX)),
            dma((2, NX)),
            dma((2, NZ, 2)),
            dma((2, NZ, 2)),
            dma((2, NX)),
            dma((2, NX)),
            dma((2, NX)),
            dma((2, NX)),
        ],
        compiler_params=pltpu.CompilerParams(
            collective_id=0, has_side_effects=True, vmem_limit_bytes=60 * 1024 * 1024
        ),
        name="delta_all",
    )(
        beta_bias,
        rate_log,
        new_beta,
        new_decay,
        tokens,
        query_weight,
        key_weight,
        value_weight,
        gate_weight,
        beta_weight.T,
        decay_weight.T,
        out_gain.reshape(1, E),
        new_query,
        new_key,
        new_value,
    )
    return pl.pallas_call(
        hand_over,
        out_shape=tuple(jax.ShapeDtypeStruct(o.shape, o.dtype) for o in out),
        in_specs=[vmem] * 3,
        out_specs=(vmem,) * 3,
        name="hand_over",
    )(*out)


def solution(mesh):
    torus = Mesh(mesh.devices.reshape(NZ, NX, NY, NC), ("z", "x", "y", "c"))
    sp, tp = ("z", "x"), ("y", "c")
    in_specs = (
        P(None, sp, tp),
        P(None, tp),
        P(None, tp),
        P(None, tp),
        P(None, tp),
        P(None, tp),
        P(None, tp),
        P(tp),
        P(tp),
        P(),
        P(None, tp, None),
        P(None, tp, None),
        P(None, tp, None),
        P(None, tp),
        P(None, tp),
    )
    out_specs = (P(None, sp, tp), P(None, tp, sp, None), P(None, tp))
    return jax.shard_map(
        shards, mesh=torus, in_specs=in_specs, out_specs=out_specs, check_vma=False
    )
```

```python
import jax
import jax.numpy as jnp
from jax import lax
from jax.experimental import pallas as pl
from jax.experimental.pallas import tpu as pltpu
from jax.sharding import Mesh
from jax.sharding import PartitionSpec as P

MESH = pl.DeviceIdType.MESH
F32 = jnp.float32
BF = jnp.bfloat16
NZ, NX, NY, NC = 8, 4, 4, 2
L = 192
HALF = L // 2
E = 128
KC = 512
D = 4096
PAD = 16
BLOCK = 64
HE = E // 2
ROWS = E + HE + PAD
PIECES = ((0, 112), (112, 96))


def dot(a, b):
    return jnp.dot(a, b, preferred_element_type=F32)


def dot_nt(a, b):
    return lax.dot_general(a, b, (((1,), (1,)), ((), ())), preferred_element_type=F32)


def dot_tn(a, b):
    return lax.dot_general(a, b, (((0,), (0,)), ((), ())), preferred_element_type=F32)


def split3(x):
    hi = x.astype(BF)
    rest = x - hi.astype(F32)
    mid = rest.astype(BF)
    low = (rest - mid.astype(F32)).astype(BF)
    return hi, mid, low


def compose(later, earlier):
    al, xl = later
    ae, xe = earlier
    grown = jnp.concatenate([ae * xl[:E], xl[E:]], axis=0)
    return al * ae, al * xe + grown - dot(xe.astype(BF), xl[:E].astype(BF))


def apply_map(m, state):
    a, x = m
    return a * state - dot(state.astype(BF), x[:E].astype(BF)) + x[E:]


def tail_rows(a):
    hi, mid, low = split3(a)
    row = lax.broadcasted_iota(jnp.int32, (PAD, E), 0)
    return jnp.where(
        row == 0,
        hi.astype(F32),
        jnp.where(row == 1, mid.astype(F32), jnp.where(row == 2, low.astype(F32), 0.0)),
    ).astype(BF)


def tail_value(rows):
    return jnp.sum(rows.astype(F32), axis=0, keepdims=True)


def kernel(
    bias_ref,
    rate_ref,
    nbeta_ref,
    ndecay_ref,
    tok_ref,
    wq_ref,
    wk_ref,
    wv_ref,
    wg_ref,
    wb_ref,
    wd_ref,
    gain_ref,
    nq_ref,
    nk_ref,
    nv_ref,
    out_ref,
    cache_ref,
    first_ref,
    xbuf,
    wbuf,
    pj,
    acc,
    wbd,
    lo,
    reach,
    sols,
    msg,
    xin,
    zin,
    ret,
    pin,
    side,
    sin,
    wsem,
    tsem,
    ys_sem,
    yr_sem,
    fs_sem,
    fr_sem,
    ps_sem,
    pr_sem,
    xs_sem,
    xr_sem,
    zs_sem,
    zr_sem,
    rs_sem,
    rr_sem,
    ss_sem,
    sr_sem,
):
    z, x, y, c = (lax.axis_index(n) for n in ("z", "x", "y", "c"))
    yu, yd = lax.rem(y + 1, NY), lax.rem(y + NY - 1, NY)
    yf = lax.rem(y + 2, NY)
    head, side_half = x // 2, lax.rem(x, 2)
    other = 1 - c

    def z_at(d):
        return lax.rem(z + d + NZ, NZ)

    def cols(yy, cc):
        return pl.ds(pl.multiple_of((yy * NC + cc) * KC, KC), KC)

    wcopies = []
    for i, w in enumerate((wq_ref, wk_ref, wv_ref, wg_ref)):
        cp = pltpu.make_async_copy(w, wbuf.at[i], wsem.at[i])
        wcopies.append(cp)
    tcopies = []
    for s in range(2):
        cp = pltpu.make_async_copy(tok_ref.at[s], xbuf.at[s, :, cols(y, c)], tsem.at[s])
        cp.start()
        tcopies.append(cp)
    for cp in wcopies:
        cp.start()

    barrier = pltpu.get_barrier_semaphore()
    partners = [{"y": yu}, {"y": yd}, {"c": other}]
    partners += [{"z": z_at(d)} for d in (1, -1, 2, -2)]
    partners += [{"x": lax.rem(x + d, NX)} for d in (1, 2, 3)]
    for p in partners:
        pl.semaphore_signal(barrier, inc=1, device_id=p, device_id_type=MESH)
    pl.semaphore_wait(barrier, len(partners))

    def ycopy(s, half, direction):
        part = xbuf.at[s, pl.ds(half * HALF, HALF), cols(y, c)]
        return pltpu.make_async_remote_copy(
            src_ref=part,
            dst_ref=part,
            send_sem=ys_sem.at[s, half, direction],
            recv_sem=yr_sem.at[s, half, direction],
            device_id={"y": yu if direction == 0 else yd},
            device_id_type=MESH,
        )

    def yarrive(s, half, direction):
        part = xbuf.at[s, pl.ds(half * HALF, HALF), cols(yd if direction == 0 else yu, c)]
        return pltpu.make_async_remote_copy(
            src_ref=part,
            dst_ref=part,
            send_sem=ys_sem.at[s, half, direction],
            recv_sem=yr_sem.at[s, half, direction],
            device_id={"y": yu if direction == 0 else yd},
            device_id_type=MESH,
        )

    def fcopy(s, direction):
        part = xbuf.at[s, pl.ds(direction * HALF, HALF), cols(yd if direction == 0 else yu, c)]
        return pltpu.make_async_remote_copy(
            src_ref=part,
            dst_ref=part,
            send_sem=fs_sem.at[s, direction],
            recv_sem=fr_sem.at[s, direction],
            device_id={"y": yu if direction == 0 else yd},
            device_id_type=MESH,
        )

    def farrive(s, direction):
        part = xbuf.at[s, pl.ds(direction * HALF, HALF), cols(yf, c)]
        return pltpu.make_async_remote_copy(
            src_ref=part,
            dst_ref=part,
            send_sem=fs_sem.at[s, direction],
            recv_sem=fr_sem.at[s, direction],
            device_id={"y": yu if direction == 0 else yd},
            device_id_type=MESH,
        )

    def pcopy(s, k, cc):
        part = xbuf.at[s, :, cols((y, yd, yu, yf)[k], cc)]
        return pltpu.make_async_remote_copy(
            src_ref=part,
            dst_ref=part,
            send_sem=ps_sem.at[s, k],
            recv_sem=pr_sem.at[s, k],
            device_id={"c": other},
            device_id_type=MESH,
        )

    def send_own(s):
        tcopies[s].wait()
        ycopy(s, 0, 0).start()
        ycopy(s, 1, 1).start()
        ycopy(s, 1, 0).start()
        ycopy(s, 0, 1).start()
        pcopy(s, 0, c).start()

    def forward(s):
        yarrive(s, 0, 0).wait_recv()
        fcopy(s, 0).start()
        yarrive(s, 1, 1).wait_recv()
        fcopy(s, 1).start()

    def near_start(s):
        yarrive(s, 1, 0).wait_recv()
        pcopy(s, 1, c).start()
        yarrive(s, 0, 1).wait_recv()
        pcopy(s, 2, c).start()

    def near_end(s):
        for k in range(3):
            pcopy(s, k, other).wait_recv()

    def far_start(s):
        farrive(s, 0).wait_recv()
        farrive(s, 1).wait_recv()
        pcopy(s, 3, c).start()

    def far_end(s):
        pcopy(s, 3, other).wait_recv()

    it = lax.broadcasted_iota(jnp.int32, (L, L), 0)
    js = lax.broadcasted_iota(jnp.int32, (L, L), 1)
    lower = it >= js
    bt = lax.broadcasted_iota(jnp.int32, (BLOCK, BLOCK), 0)
    bs = lax.broadcasted_iota(jnp.int32, (BLOCK, BLOCK), 1)

    def project(s, which):
        for i in which:
            pj[s, i] = dot(xbuf[s], wbuf[i]).astype(BF)

    def chip(yy):
        return pl.ds(pl.multiple_of(yy * NC * KC, NC * KC), NC * KC)

    def near(s):
        for n, i in enumerate((1, 2)):
            acc[n] = sum(dot(xbuf[s, :, chip(q)], wbuf[i, chip(q), :]) for q in (y, yd, yu))
        return sum(dot(xbuf[s, :, chip(q)], wbd[chip(q), :]) for q in (y, yd, yu))

    def far(s, part):
        for n, i in enumerate((1, 2)):
            pj[s, i] = (acc[n] + dot(xbuf[s, :, chip(yf)], wbuf[i, chip(yf), :])).astype(BF)
        return part + dot(xbuf[s, :, chip(yf)], wbd[chip(yf), :])

    heads = range(2)

    def scale(v):
        v = v.astype(F32)
        return lax.rsqrt(jnp.sum(v * v, axis=1, keepdims=True) + 1.0)

    def head_of(s, i, h):
        return pj[s, i, :, h * E : (h + 1) * E]

    def chain_terms(s, bd, between, ending):
        lane = lax.broadcasted_iota(jnp.int32, (L, PAD), 1)
        bias = jnp.where(lane == 0, bias_ref[0], jnp.where(lane == 1, bias_ref[1], 0.0))
        rate = jnp.where(lane == 2, rate_ref[0], jnp.where(lane == 3, rate_ref[1], 0.0))
        beta = jax.nn.sigmoid(bd + bias)
        soft = jnp.maximum(bd, 0.0) + jnp.log1p(jnp.exp(-jnp.abs(bd)))
        g = -jnp.exp(rate) * soft
        tri = jnp.where(lower, 1.0, 0.0).astype(BF)
        cum = sum(dot(tri, part) for part in split3(g))
        ks = [head_of(s, 1, h) for h in heads]
        vs = [head_of(s, 2, h) for h in heads]
        rk = [scale(v) for v in ks]
        pack = jnp.where(lane == 0, rk[0], jnp.where(lane == 1, rk[1], cum))
        eye = jnp.where(
            lax.broadcasted_iota(jnp.int32, (PAD, PAD), 0)
            == lax.broadcasted_iota(jnp.int32, (PAD, PAD), 1),
            1.0,
            0.0,
        ).astype(BF)
        rows = sum(dot_nt(eye, part) for part in split3(pack))
        cumc = [cum[:, 2 + h : 3 + h] for h in heads]
        betac = [beta[:, h : h + 1] for h in heads]

        def corner(h, top, count, left):
            span = slice(top, top + count)
            kk = dot_nt(ks[h][span], ks[h][left : left + BLOCK])
            gap = cumc[h][span] - rows[2 + h : 3 + h, left : left + BLOCK]
            if top == left:
                gap = jnp.where(bt > bs, gap, 0.0)
            value = kk * (betac[h] * rk[h])[span] * jnp.exp(gap) * rows[h : h + 1, left : left + BLOCK]
            return jnp.where(bt > bs, value, 0.0) if top == left else value

        def level_mask(bit):
            return ((bt >> (bit + 1)) == (bs >> (bit + 1))) & ((bt >> bit) != (bs >> bit))

        diag = [corner(h, BLOCK * n, BLOCK, BLOCK * n) for h in heads for n in range(3)]
        m = level_mask(0)
        invs = [-jnp.where(m, a, 0.0) for a in diag]
        for bit in range(1, 6):
            m = level_mask(bit)
            halfway = []
            for a, inv in zip(diag, invs):
                off = jnp.where(m, a, 0.0)
                halfway.append(off + dot(off.astype(BF), inv.astype(BF)))
            invs = [
                inv - yy - dot(inv.astype(BF), yy.astype(BF)) for inv, yy in zip(invs, halfway)
            ]
        invs = [inv.astype(BF) for inv in invs]
        between()
        rhs, sols_of = [], [[], []]
        for h in heads:
            kf = ks[h].astype(F32)
            rhs.append(
                jnp.concatenate(
                    [
                        kf * (betac[h] * rk[h] * jnp.exp(cumc[h])),
                        vs[h].astype(F32) * betac[h],
                    ],
                    axis=1,
                )
            )
        rest = rhs
        for n in range(3):
            for h in heads:
                now = rest[h][:BLOCK]
                sols_of[h].append((now + dot(invs[3 * h + n], now.astype(BF))).astype(BF))
            if n < 2:
                rest = [
                    rest[h][BLOCK:]
                    - dot(
                        corner(h, BLOCK * (n + 1), L - BLOCK * (n + 1), BLOCK * n).astype(BF),
                        sols_of[h][n],
                    )
                    for h in heads
                ]
        ending()
        for h in heads:
            b = 2 * s + h
            kf = ks[h].astype(F32)
            sb = jnp.concatenate(sols_of[h], axis=0)
            last = cumc[h][L - 1 : L, :]
            kd = kf * (rk[h] * jnp.exp(last - cumc[h]))
            rs = dot_tn(sb, kd.astype(BF)).astype(BF)
            msg[s, h, 0:HE, :] = rs[E : E + HE]
            msg[s, h, HE : HE + E, :] = rs[:E]
            msg[s, h, HE + E : ROWS, :] = tail_rows(jnp.broadcast_to(jnp.exp(last), (1, E)))
            msg[s, h, ROWS:, :] = rs[E + HE :]
            sols[b] = sb
        return cumc, rows

    def out_terms(s, cumc, rows):
        for h in heads:
            b = 2 * s + h
            q, k = head_of(s, 0, h), head_of(s, 1, h)
            rq = scale(q)
            cc = cumc[h]
            decay = jnp.exp(jnp.where(lower, cc - rows[2 + h : 3 + h, :], 0.0)) * rows[h : h + 1, :]
            score = jnp.where(lower, dot_nt(q, k) * rq * decay, 0.0).astype(BF)
            sx = dot(score, sols[b])
            lo[b] = sx[:, E:]
            qd = q.astype(F32) * (rq * jnp.exp(cc))
            reach[b] = (qd - sx[:, :E]).astype(BF)

    def xpart(s, t):
        return msg.at[s, t // 2, pl.ds(HE * (t % 2), ROWS)]

    def xcopy(s, t, src_x):
        return pltpu.make_async_remote_copy(
            src_ref=xpart(s, t),
            dst_ref=xin.at[s, src_x],
            send_sem=xs_sem.at[s, t],
            recv_sem=xr_sem.at[s, src_x],
            device_id={"x": t},
            device_id_type=MESH,
        )

    def xlocal(s, t):
        return pltpu.make_async_copy(xpart(s, t), xin.at[s, t], xs_sem.at[s, t])

    def spread(remote, local):
        for t in range(NX):

            @pl.when(x != t)
            def _():
                remote(t).start()

            @pl.when(x == t)
            def _():
                local(t).start()

    def collect(remote, local):
        for t in range(NX):

            @pl.when(x != t)
            def _():
                remote(t).wait_recv()

            @pl.when(x == t)
            def _():
                local(t).wait()

    def xsend(s):
        spread(lambda t: xcopy(s, t, x), lambda t: xlocal(s, t))

    def zcopy(s, slot, piece, hop, dist):
        first, count = PIECES[piece]
        part = zin.at[s, slot, pl.ds(first, count)]
        return pltpu.make_async_remote_copy(
            src_ref=part,
            dst_ref=part,
            send_sem=zs_sem.at[s, dist % NZ, piece],
            recv_sem=zr_sem.at[s, dist % NZ, piece],
            device_id={"z": z_at(hop)},
            device_id_type=MESH,
        )

    def zsend(s):
        collect(lambda t: xcopy(s, t, t), lambda t: xlocal(s, t))
        maps = []
        for j in range(NX):
            r = xin[s, j, pl.ds(pl.multiple_of(HE * (1 - side_half), PAD), E), :]
            a = xin[s, j, pl.ds(pl.multiple_of(E + HE - HE * side_half, PAD), PAD), :]
            v = xin[s, j, pl.ds(pl.multiple_of((E + PAD) * side_half, PAD), HE), :]
            maps.append((tail_value(a), jnp.concatenate([r, v], axis=0).astype(F32)))
        m10 = compose(maps[1], maps[0])
        m32 = compose(maps[3], maps[2])
        a, total = compose(m32, m10)
        zin[s, z, 0 : E + HE, :] = total.astype(BF)
        zin[s, z, E + HE : ROWS, :] = tail_rows(a)
        for hop in (2, -2, 1, -1):
            for piece in range(2):
                zcopy(s, z, piece, hop, hop).start()
        return maps[0], m10, maps[2]

    def zrelay(s):
        for piece in range(2):
            for d in (1, -1):
                slot = z_at(-2 * d)
                zcopy(s, slot, piece, 1, 2 * d).wait_recv()
                zcopy(s, slot, piece, d, 3 * d).start()
                if (piece == 0) == (d == 1):
                    zcopy(s, slot, piece, 2 * d, 4).start()

    def zwait(s, *dists):
        for d in dists:
            for piece in range(2):
                zcopy(s, z_at(-d), piece, 1, d).wait_recv()

    def zmap(s, slot):
        return tail_value(zin[s, slot, E + HE : ROWS, :]), zin[s, slot, 0 : E + HE, :].astype(F32)

    def zmap_if(s, d):
        valid = z + d >= NZ if d > 0 else z + d >= 0
        a, m = zmap(s, z_at(d))
        return jnp.where(valid, a, 1.0), jnp.where(valid, m, 0.0)

    def rcopy(s, t, src_x):
        return pltpu.make_async_remote_copy(
            src_ref=ret.at[s, t],
            dst_ref=pin.at[s, src_x],
            send_sem=rs_sem.at[s, t],
            recv_sem=rr_sem.at[s, src_x],
            device_id={"x": t},
            device_id_type=MESH,
        )

    def rlocal(s, t):
        return pltpu.make_async_copy(ret.at[s, t], pin.at[s, t], rs_sem.at[s, t])

    def scopy(s, t, src_x):
        return pltpu.make_async_remote_copy(
            src_ref=side.at[s, t],
            dst_ref=sin.at[s, src_x],
            send_sem=ss_sem.at[s, t],
            recv_sem=sr_sem.at[s, src_x],
            device_id={"x": t},
            device_id_type=MESH,
        )

    def slocal(s, t):
        return pltpu.make_async_copy(side.at[s, t], sin.at[s, t], ss_sem.at[s, t])

    def start_states(s, inner):
        m0, m10, m2 = inner
        m210 = compose(m2, m10)
        zwait(s, 1, -1)
        behind = compose(zmap_if(s, -1), zmap_if(s, -2))
        early = apply_map(zmap_if(s, 2), zmap_if(s, 1)[1][E:])
        zwait(s, 3, -3, 4)
        behind = compose(behind, zmap_if(s, -3))
        early = apply_map(zmap_if(s, -4), apply_map(zmap_if(s, 3), early))
        here = apply_map(behind, early)
        ret_of = [here] + [apply_map(m, here) for m in (m0, m10, m210)]
        for t in range(NX):
            ret[s, t] = ret_of[t].astype(BF)
        spread(lambda t: rcopy(s, t, x), lambda t: rlocal(s, t))

    def unit(v):
        return v * lax.rsqrt(jnp.sum(v * v, axis=1, keepdims=True) + 1.0)

    gain = gain_ref[...]

    def final_parts(s):
        state = apply_map(zmap(s, 1), zmap(s, 0)[1][E:])
        for k in (2, 4, 6):
            state = apply_map(compose(zmap(s, k + 1), zmap(s, k)), state)
        place = lax.broadcasted_iota(jnp.int32, (HE, E), 1) == (
            lax.broadcasted_iota(jnp.int32, (HE, E), 0) + HE * side_half
        )
        memf = dot_tn(state.astype(BF), jnp.where(place, 1.0, 0.0).astype(BF))
        memory = memf.astype(BF)

        def pick(ref):
            row = ref[s].astype(F32)
            return jnp.where(head == 0, row[0:1, :], row[1:2, :])

        qn, kn, nv = unit(pick(nq_ref)), unit(pick(nk_ref)), pick(nv_ref)
        nbeta = jnp.where(head == 0, nbeta_ref[s, 0], nbeta_ref[s, 1])
        ndecay = jnp.where(head == 0, ndecay_ref[s, 0], ndecay_ref[s, 1])
        row = lax.broadcasted_iota(jnp.int32, (PAD, E), 0)
        asked = jnp.where(row == 0, qn, jnp.where(row == 1, kn, 0.0))
        seen = sum(dot(part, memory) for part in split3(asked))
        recall, retrieve = seen[0:1, :], seen[1:2, :]
        intersect = jnp.sum(kn * qn, axis=1, keepdims=True)
        lane = lax.broadcasted_iota(jnp.int32, (1, E), 1)
        nv = jnp.where((lane >= HE) == (side_half == 1), nv, 0.0)
        fresh = nv - ndecay * retrieve
        read = ndecay * recall + (nbeta * intersect) * fresh
        mine = memf[0:16, :]
        for k in range(1, NZ):
            mine = jnp.where(z == k, memf[16 * k : 16 * k + 16, :], mine)
        for t in range(NX):
            side[s, t, 0:4, :] = mine[4 * t : 4 * t + 4, :]
            side[s, t, 4:8, :] = jnp.broadcast_to(read, (4, E))
        spread(lambda t: scopy(s, t, x), lambda t: slocal(s, t))

    def outputs(s):
        collect(lambda t: rcopy(s, t, t), lambda t: rlocal(s, t))
        for h in heads:
            b = 2 * s + h
            start = jnp.concatenate([pin[s, 2 * h], pin[s, 2 * h + 1]], axis=0)
            o = lo[b] + dot_nt(reach[b], start)
            gate = head_of(s, 3, h).astype(F32)
            norm = lax.rsqrt(jnp.mean(o * o, axis=1, keepdims=True) + 0.001)
            out_ref[s, :, h * E : (h + 1) * E] = (
                o * norm * gain * (gate * jax.nn.sigmoid(gate))
            ).astype(BF)

    def last_parts(s):
        collect(lambda t: scopy(s, t, t), lambda t: slocal(s, t))
        for h in heads:
            both = sin[s, 2 * h] + sin[s, 2 * h + 1]
            cache_ref[s, h] = both[0:4].astype(BF)
            read = both[4:5]
            norm = lax.rsqrt(jnp.mean(read * read, axis=1, keepdims=True) + 0.001)
            first_ref[s : s + 1, h * E : (h + 1) * E] = read * norm * gain

    inner = []
    send_own(0)
    small_rows = jnp.concatenate(
        [wb_ref[...].astype(F32), wd_ref[...].astype(F32), jnp.zeros((PAD - 4, D), F32)], axis=0
    )
    wbd[...] = small_rows.T.astype(BF)
    forward(0)
    send_own(1)
    near_start(0)
    near_end(0)
    far_start(0)
    for cp in wcopies:
        cp.wait()
    part = near(0)
    forward(1)
    far_end(0)
    kept0 = chain_terms(0, far(0, part), lambda: near_start(1), lambda: far_start(1))
    xsend(0)
    near_end(1)
    part = near(1)
    far_end(1)
    kept1 = chain_terms(1, far(1, part), lambda: inner.append(zsend(0)), lambda: None)
    xsend(1)
    project(0, (0, 3))
    out_terms(0, *kept0)
    project(1, (0, 3))
    zrelay(0)
    out_terms(1, *kept1)
    inner.append(zsend(1))
    zrelay(1)
    start_states(0, inner[0])
    final_parts(0)
    start_states(1, inner[1])
    final_parts(1)
    outputs(0)
    last_parts(0)
    outputs(1)
    last_parts(1)

    for s in range(2):
        for half in range(2):
            for direction in range(2):
                ycopy(s, half, direction).wait_send()
        for direction in range(2):
            fcopy(s, direction).wait_send()
        for k in range(4):
            pcopy(s, k, c).wait_send()
        for t in range(NX):

            @pl.when(x != t)
            def _():
                xcopy(s, t, x).wait_send()
                rcopy(s, t, x).wait_send()
                scopy(s, t, x).wait_send()

        for hop in (2, -2, 1, -1):
            for piece in range(2):
                zcopy(s, z, piece, hop, hop).wait_send()
        for piece in range(2):
            for d in (1, -1):
                zcopy(s, z_at(-2 * d), piece, d, 3 * d).wait_send()
                if (piece == 0) == (d == 1):
                    zcopy(s, z_at(-2 * d), piece, 2 * d, 4).wait_send()


def hand_over(mixed_in, cache_in, first_in, mixed_out, cache_out, first_out):
    mixed_out[...] = mixed_in[...]
    cache_out[...] = cache_in[...]
    first_out[...] = first_in[...]


def shards(
    tokens,
    query_weight,
    key_weight,
    value_weight,
    gate_weight,
    beta_weight,
    decay_weight,
    beta_bias,
    rate_log,
    out_gain,
    new_query,
    new_key,
    new_value,
    new_beta,
    new_decay,
):
    smem = pl.BlockSpec(memory_space=pltpu.SMEM)
    vmem = pl.BlockSpec(memory_space=pltpu.VMEM)
    hbm = pl.BlockSpec(memory_space=pl.ANY)
    dma = pltpu.SemaphoreType.DMA
    out = pl.pallas_call(
        kernel,
        out_shape=(
            jax.ShapeDtypeStruct((2, L, 2 * E), BF),
            jax.ShapeDtypeStruct((2, 2, 4, E), BF),
            jax.ShapeDtypeStruct((2, 2 * E), F32),
        ),
        in_specs=[smem] * 4 + [hbm] * 5 + [vmem] * 6,
        out_specs=(vmem, vmem, vmem),
        scratch_shapes=[
            pltpu.VMEM((2, L, D), BF),
            pltpu.VMEM((4, D, 2 * E), BF),
            pltpu.VMEM((2, 4, L, 2 * E), BF),
            pltpu.VMEM((2, L, 2 * E), F32),
            pltpu.VMEM((D, PAD), BF),
            pltpu.VMEM((4, L, E), F32),
            pltpu.VMEM((4, L, E), BF),
            pltpu.VMEM((4, L, 2 * E), BF),
            pltpu.VMEM((2, 2, E + 2 * HE + PAD, E), BF),
            pltpu.VMEM((2, NX, ROWS, E), BF),
            pltpu.VMEM((2, NZ, ROWS, E), BF),
            pltpu.VMEM((2, NX, HE, E), BF),
            pltpu.VMEM((2, NX, HE, E), BF),
            pltpu.VMEM((2, NX, 8, E), F32),
            pltpu.VMEM((2, NX, 8, E), F32),
            dma((4,)),
            dma((2,)),
            dma((2, 2, 2)),
            dma((2, 2, 2)),
            dma((2, 2)),
            dma((2, 2)),
            dma((2, 4)),
            dma((2, 4)),
            dma((2, NX)),
            dma((2, NX)),
            dma((2, NZ, 2)),
            dma((2, NZ, 2)),
            dma((2, NX)),
            dma((2, NX)),
            dma((2, NX)),
            dma((2, NX)),
        ],
        compiler_params=pltpu.CompilerParams(
            collective_id=0, has_side_effects=True, vmem_limit_bytes=60 * 1024 * 1024
        ),
        name="delta_all",
    )(
        beta_bias,
        rate_log,
        new_beta,
        new_decay,
        tokens,
        query_weight,
        key_weight,
        value_weight,
        gate_weight,
        beta_weight.T,
        decay_weight.T,
        out_gain.reshape(1, E),
        new_query,
        new_key,
        new_value,
    )
    return pl.pallas_call(
        hand_over,
        out_shape=tuple(jax.ShapeDtypeStruct(o.shape, o.dtype) for o in out),
        in_specs=[vmem] * 3,
        out_specs=(vmem,) * 3,
        name="hand_over",
    )(*out)


def solution(mesh):
    torus = Mesh(mesh.devices.reshape(NZ, NX, NY, NC), ("z", "x", "y", "c"))
    sp, tp = ("z", "x"), ("y", "c")
    in_specs = (
        P(None, sp, tp),
        P(None, tp),
        P(None, tp),
        P(None, tp),
        P(None, tp),
        P(None, tp),
        P(None, tp),
        P(tp),
        P(tp),
        P(),
        P(None, tp, None),
        P(None, tp, None),
        P(None, tp, None),
        P(None, tp),
        P(None, tp),
    )
    out_specs = (P(None, sp, tp), P(None, tp, sp, None), P(None, tp))
    return jax.shard_map(
        shards, mesh=torus, in_specs=in_specs, out_specs=out_specs, check_vma=False
    )
```

```python
import jax
import jax.numpy as jnp
from jax import lax
from jax.experimental import pallas as pl
from jax.experimental.pallas import tpu as pltpu
from jax.sharding import Mesh
from jax.sharding import PartitionSpec as P

MESH = pl.DeviceIdType.MESH
F32 = jnp.float32
BF = jnp.bfloat16
NZ, NX, NY, NC = 8, 4, 4, 2
L = 192
HALF = L // 2
E = 128
KC = 512
D = 4096
PAD = 16
BLOCK = 64
HE = E // 2
ROWS = E + HE + PAD
PIECES = ((0, 112), (112, 96))


def dot(a, b):
    return jnp.dot(a, b, preferred_element_type=F32)


def dot_nt(a, b):
    return lax.dot_general(a, b, (((1,), (1,)), ((), ())), preferred_element_type=F32)


def dot_tn(a, b):
    return lax.dot_general(a, b, (((0,), (0,)), ((), ())), preferred_element_type=F32)


def split3(x):
    hi = x.astype(BF)
    rest = x - hi.astype(F32)
    mid = rest.astype(BF)
    low = (rest - mid.astype(F32)).astype(BF)
    return hi, mid, low


def compose(later, earlier):
    al, xl = later
    ae, xe = earlier
    grown = jnp.concatenate([ae * xl[:E], xl[E:]], axis=0)
    return al * ae, al * xe + grown - dot(xe.astype(BF), xl[:E].astype(BF))


def apply_map(m, state):
    a, x = m
    return a * state - dot(state.astype(BF), x[:E].astype(BF)) + x[E:]


def tail_rows(a):
    hi, mid, low = split3(a)
    row = lax.broadcasted_iota(jnp.int32, (PAD, E), 0)
    return jnp.where(
        row == 0,
        hi.astype(F32),
        jnp.where(row == 1, mid.astype(F32), jnp.where(row == 2, low.astype(F32), 0.0)),
    ).astype(BF)


def tail_value(rows):
    return jnp.sum(rows.astype(F32), axis=0, keepdims=True)


def kernel(
    bias_ref,
    rate_ref,
    nbeta_ref,
    ndecay_ref,
    tok_ref,
    wq_ref,
    wk_ref,
    wv_ref,
    wg_ref,
    wb_ref,
    wd_ref,
    gain_ref,
    nq_ref,
    nk_ref,
    nv_ref,
    out_ref,
    cache_ref,
    first_ref,
    xbuf,
    wbuf,
    pj,
    acc,
    wbd,
    lo,
    reach,
    sols,
    msg,
    xin,
    zin,
    ret,
    pin,
    side,
    sin,
    wsem,
    tsem,
    ys_sem,
    yr_sem,
    fs_sem,
    fr_sem,
    ps_sem,
    pr_sem,
    xs_sem,
    xr_sem,
    zs_sem,
    zr_sem,
    rs_sem,
    rr_sem,
    ss_sem,
    sr_sem,
):
    z, x, y, c = (lax.axis_index(n) for n in ("z", "x", "y", "c"))
    yu, yd = lax.rem(y + 1, NY), lax.rem(y + NY - 1, NY)
    yf = lax.rem(y + 2, NY)
    head, side_half = x // 2, lax.rem(x, 2)
    other = 1 - c

    def z_at(d):
        return lax.rem(z + d + NZ, NZ)

    def cols(yy, cc):
        return pl.ds(pl.multiple_of((yy * NC + cc) * KC, KC), KC)

    wcopies = []
    for i, w in enumerate((wq_ref, wk_ref, wv_ref, wg_ref)):
        cp = pltpu.make_async_copy(w, wbuf.at[i], wsem.at[i])
        wcopies.append(cp)
    tcopies = []
    for s in range(2):
        cp = pltpu.make_async_copy(tok_ref.at[s], xbuf.at[s, :, cols(y, c)], tsem.at[s])
        cp.start()
        tcopies.append(cp)
    for cp in wcopies:
        cp.start()

    barrier = pltpu.get_barrier_semaphore()
    partners = [{"y": yu}, {"y": yd}, {"c": other}]
    partners += [{"z": z_at(d)} for d in (1, -1, 2, -2)]
    partners += [{"x": lax.rem(x + d, NX)} for d in (1, 2, 3)]
    for p in partners:
        pl.semaphore_signal(barrier, inc=1, device_id=p, device_id_type=MESH)
    pl.semaphore_wait(barrier, len(partners))

    def ycopy(s, half, direction):
        part = xbuf.at[s, pl.ds(half * HALF, HALF), cols(y, c)]
        return pltpu.make_async_remote_copy(
            src_ref=part,
            dst_ref=part,
            send_sem=ys_sem.at[s, half, direction],
            recv_sem=yr_sem.at[s, half, direction],
            device_id={"y": yu if direction == 0 else yd},
            device_id_type=MESH,
        )

    def yarrive(s, half, direction):
        part = xbuf.at[s, pl.ds(half * HALF, HALF), cols(yd if direction == 0 else yu, c)]
        return pltpu.make_async_remote_copy(
            src_ref=part,
            dst_ref=part,
            send_sem=ys_sem.at[s, half, direction],
            recv_sem=yr_sem.at[s, half, direction],
            device_id={"y": yu if direction == 0 else yd},
            device_id_type=MESH,
        )

    def fcopy(s, direction):
        part = xbuf.at[s, pl.ds(direction * HALF, HALF), cols(yd if direction == 0 else yu, c)]
        return pltpu.make_async_remote_copy(
            src_ref=part,
            dst_ref=part,
            send_sem=fs_sem.at[s, direction],
            recv_sem=fr_sem.at[s, direction],
            device_id={"y": yu if direction == 0 else yd},
            device_id_type=MESH,
        )

    def farrive(s, direction):
        part = xbuf.at[s, pl.ds(direction * HALF, HALF), cols(yf, c)]
        return pltpu.make_async_remote_copy(
            src_ref=part,
            dst_ref=part,
            send_sem=fs_sem.at[s, direction],
            recv_sem=fr_sem.at[s, direction],
            device_id={"y": yu if direction == 0 else yd},
            device_id_type=MESH,
        )

    def pcopy(s, k, cc):
        part = xbuf.at[s, :, cols((y, yd, yu, yf)[k], cc)]
        return pltpu.make_async_remote_copy(
            src_ref=part,
            dst_ref=part,
            send_sem=ps_sem.at[s, k],
            recv_sem=pr_sem.at[s, k],
            device_id={"c": other},
            device_id_type=MESH,
        )

    def send_own(s):
        tcopies[s].wait()
        ycopy(s, 0, 0).start()
        ycopy(s, 1, 1).start()
        ycopy(s, 1, 0).start()
        ycopy(s, 0, 1).start()
        pcopy(s, 0, c).start()

    def forward(s):
        yarrive(s, 0, 0).wait_recv()
        fcopy(s, 0).start()
        yarrive(s, 1, 1).wait_recv()
        fcopy(s, 1).start()

    def near_start(s):
        yarrive(s, 1, 0).wait_recv()
        pcopy(s, 1, c).start()
        yarrive(s, 0, 1).wait_recv()
        pcopy(s, 2, c).start()

    def near_end(s):
        for k in range(3):
            pcopy(s, k, other).wait_recv()

    def far_start(s):
        farrive(s, 0).wait_recv()
        farrive(s, 1).wait_recv()
        pcopy(s, 3, c).start()

    def far_end(s):
        pcopy(s, 3, other).wait_recv()

    it = lax.broadcasted_iota(jnp.int32, (L, L), 0)
    js = lax.broadcasted_iota(jnp.int32, (L, L), 1)
    lower = it >= js
    bt = lax.broadcasted_iota(jnp.int32, (BLOCK, BLOCK), 0)
    bs = lax.broadcasted_iota(jnp.int32, (BLOCK, BLOCK), 1)

    def project(s, which):
        for i in which:
            pj[s, i] = dot(xbuf[s], wbuf[i]).astype(BF)

    def chip(yy):
        return pl.ds(pl.multiple_of(yy * NC * KC, NC * KC), NC * KC)

    def near(s):
        for n, i in enumerate((1, 2)):
            acc[n] = sum(dot(xbuf[s, :, chip(q)], wbuf[i, chip(q), :]) for q in (y, yd, yu))
        return sum(dot(xbuf[s, :, chip(q)], wbd[chip(q), :]) for q in (y, yd, yu))

    def far(s, part):
        for n, i in enumerate((1, 2)):
            pj[s, i] = (acc[n] + dot(xbuf[s, :, chip(yf)], wbuf[i, chip(yf), :])).astype(BF)
        return part + dot(xbuf[s, :, chip(yf)], wbd[chip(yf), :])

    heads = range(2)

    def scale(v):
        v = v.astype(F32)
        return lax.rsqrt(jnp.sum(v * v, axis=1, keepdims=True) + 1.0)

    def head_of(s, i, h):
        return pj[s, i, :, h * E : (h + 1) * E]

    def chain_terms(s, bd, between, ending):
        lane = lax.broadcasted_iota(jnp.int32, (L, PAD), 1)
        bias = jnp.where(lane == 0, bias_ref[0], jnp.where(lane == 1, bias_ref[1], 0.0))
        rate = jnp.where(lane == 2, rate_ref[0], jnp.where(lane == 3, rate_ref[1], 0.0))
        beta = jax.nn.sigmoid(bd + bias)
        soft = jnp.maximum(bd, 0.0) + jnp.log1p(jnp.exp(-jnp.abs(bd)))
        g = -jnp.exp(rate) * soft
        tri = jnp.where(lower, 1.0, 0.0).astype(BF)
        cum = sum(dot(tri, part) for part in split3(g))
        ks = [head_of(s, 1, h) for h in heads]
        vs = [head_of(s, 2, h) for h in heads]
        rk = [scale(v) for v in ks]
        pack = jnp.where(lane == 0, rk[0], jnp.where(lane == 1, rk[1], cum))
        eye = jnp.where(
            lax.broadcasted_iota(jnp.int32, (PAD, PAD), 0)
            == lax.broadcasted_iota(jnp.int32, (PAD, PAD), 1),
            1.0,
            0.0,
        ).astype(BF)
        rows = sum(dot_nt(eye, part) for part in split3(pack))
        cumc = [cum[:, 2 + h : 3 + h] for h in heads]
        betac = [beta[:, h : h + 1] for h in heads]

        def corner(h, top, count, left):
            span = slice(top, top + count)
            kk = dot_nt(ks[h][span], ks[h][left : left + BLOCK])
            gap = cumc[h][span] - rows[2 + h : 3 + h, left : left + BLOCK]
            if top == left:
                gap = jnp.where(bt > bs, gap, 0.0)
            value = kk * (betac[h] * rk[h])[span] * jnp.exp(gap) * rows[h : h + 1, left : left + BLOCK]
            return jnp.where(bt > bs, value, 0.0) if top == left else value

        def level_mask(bit):
            return ((bt >> (bit + 1)) == (bs >> (bit + 1))) & ((bt >> bit) != (bs >> bit))

        diag = [corner(h, BLOCK * n, BLOCK, BLOCK * n) for h in heads for n in range(3)]
        m = level_mask(0)
        invs = [-jnp.where(m, a, 0.0) for a in diag]
        for bit in range(1, 6):
            m = level_mask(bit)
            halfway = []
            for a, inv in zip(diag, invs):
                off = jnp.where(m, a, 0.0)
                halfway.append(off + dot(off.astype(BF), inv.astype(BF)))
            invs = [
                inv - yy - dot(inv.astype(BF), yy.astype(BF)) for inv, yy in zip(invs, halfway)
            ]
        invs = [inv.astype(BF) for inv in invs]
        between()
        rhs, sols_of = [], [[], []]
        for h in heads:
            kf = ks[h].astype(F32)
            rhs.append(
                jnp.concatenate(
                    [
                        kf * (betac[h] * rk[h] * jnp.exp(cumc[h])),
                        vs[h].astype(F32) * betac[h],
                    ],
                    axis=1,
                )
            )
        rest = rhs
        for n in range(3):
            for h in heads:
                now = rest[h][:BLOCK]
                sols_of[h].append((now + dot(invs[3 * h + n], now.astype(BF))).astype(BF))
            if n < 2:
                rest = [
                    rest[h][BLOCK:]
                    - dot(
                        corner(h, BLOCK * (n + 1), L - BLOCK * (n + 1), BLOCK * n).astype(BF),
                        sols_of[h][n],
                    )
                    for h in heads
                ]
        ending()
        for h in heads:
            b = 2 * s + h
            kf = ks[h].astype(F32)
            sb = jnp.concatenate(sols_of[h], axis=0)
            last = cumc[h][L - 1 : L, :]
            kd = kf * (rk[h] * jnp.exp(last - cumc[h]))
            rs = dot_tn(sb, kd.astype(BF)).astype(BF)
            msg[s, h, 0:HE, :] = rs[E : E + HE]
            msg[s, h, HE : HE + E, :] = rs[:E]
            msg[s, h, HE + E : ROWS, :] = tail_rows(jnp.broadcast_to(jnp.exp(last), (1, E)))
            msg[s, h, ROWS:, :] = rs[E + HE :]
            sols[b] = sb
        return cumc, rows

    def out_terms(s, cumc, rows):
        for h in heads:
            b = 2 * s + h
            q, k = head_of(s, 0, h), head_of(s, 1, h)
            rq = scale(q)
            cc = cumc[h]
            decay = jnp.exp(jnp.where(lower, cc - rows[2 + h : 3 + h, :], 0.0)) * rows[h : h + 1, :]
            score = jnp.where(lower, dot_nt(q, k) * rq * decay, 0.0).astype(BF)
            sx = dot(score, sols[b])
            lo[b] = sx[:, E:]
            qd = q.astype(F32) * (rq * jnp.exp(cc))
            reach[b] = (qd - sx[:, :E]).astype(BF)

    def xpart(s, t):
        return msg.at[s, t // 2, pl.ds(HE * (t % 2), ROWS)]

    def xcopy(s, t, src_x):
        return pltpu.make_async_remote_copy(
            src_ref=xpart(s, t),
            dst_ref=xin.at[s, src_x],
            send_sem=xs_sem.at[s, t],
            recv_sem=xr_sem.at[s, src_x],
            device_id={"x": t},
            device_id_type=MESH,
        )

    def xlocal(s, t):
        return pltpu.make_async_copy(xpart(s, t), xin.at[s, t], xs_sem.at[s, t])

    def spread(remote, local):
        for t in range(NX):

            @pl.when(x != t)
            def _():
                remote(t).start()

            @pl.when(x == t)
            def _():
                local(t).start()

    def collect(remote, local):
        for t in range(NX):

            @pl.when(x != t)
            def _():
                remote(t).wait_recv()

            @pl.when(x == t)
            def _():
                local(t).wait()

    def xsend(s):
        spread(lambda t: xcopy(s, t, x), lambda t: xlocal(s, t))

    def zcopy(s, slot, piece, hop, dist):
        first, count = PIECES[piece]
        part = zin.at[s, slot, pl.ds(first, count)]
        return pltpu.make_async_remote_copy(
            src_ref=part,
            dst_ref=part,
            send_sem=zs_sem.at[s, dist % NZ, piece],
            recv_sem=zr_sem.at[s, dist % NZ, piece],
            device_id={"z": z_at(hop)},
            device_id_type=MESH,
        )

    def zsend(s):
        collect(lambda t: xcopy(s, t, t), lambda t: xlocal(s, t))
        maps = []
        for j in range(NX):
            r = xin[s, j, pl.ds(pl.multiple_of(HE * (1 - side_half), PAD), E), :]
            a = xin[s, j, pl.ds(pl.multiple_of(E + HE - HE * side_half, PAD), PAD), :]
            v = xin[s, j, pl.ds(pl.multiple_of((E + PAD) * side_half, PAD), HE), :]
            maps.append((tail_value(a), jnp.concatenate([r, v], axis=0).astype(F32)))
        m10 = compose(maps[1], maps[0])
        m32 = compose(maps[3], maps[2])
        a, total = compose(m32, m10)
        zin[s, z, 0 : E + HE, :] = total.astype(BF)
        zin[s, z, E + HE : ROWS, :] = tail_rows(a)
        for hop in (2, -2, 1, -1):
            for piece in range(2):
                zcopy(s, z, piece, hop, hop).start()
        return maps[0], m10, maps[2]

    def zrelay(s):
        for piece in range(2):
            for d in (1, -1):
                slot = z_at(-2 * d)
                zcopy(s, slot, piece, 1, 2 * d).wait_recv()
                zcopy(s, slot, piece, d, 3 * d).start()
                if (piece == 0) == (d == 1):
                    zcopy(s, slot, piece, 2 * d, 4).start()

    def zwait(s, *dists):
        for d in dists:
            for piece in range(2):
                zcopy(s, z_at(-d), piece, 1, d).wait_recv()

    def zmap(s, slot):
        return tail_value(zin[s, slot, E + HE : ROWS, :]), zin[s, slot, 0 : E + HE, :].astype(F32)

    def zmap_if(s, d):
        valid = z + d >= NZ if d > 0 else z + d >= 0
        a, m = zmap(s, z_at(d))
        return jnp.where(valid, a, 1.0), jnp.where(valid, m, 0.0)

    def rcopy(s, t, src_x):
        return pltpu.make_async_remote_copy(
            src_ref=ret.at[s, t],
            dst_ref=pin.at[s, src_x],
            send_sem=rs_sem.at[s, t],
            recv_sem=rr_sem.at[s, src_x],
            device_id={"x": t},
            device_id_type=MESH,
        )

    def rlocal(s, t):
        return pltpu.make_async_copy(ret.at[s, t], pin.at[s, t], rs_sem.at[s, t])

    def scopy(s, t, src_x):
        return pltpu.make_async_remote_copy(
            src_ref=side.at[s, t],
            dst_ref=sin.at[s, src_x],
            send_sem=ss_sem.at[s, t],
            recv_sem=sr_sem.at[s, src_x],
            device_id={"x": t},
            device_id_type=MESH,
        )

    def slocal(s, t):
        return pltpu.make_async_copy(side.at[s, t], sin.at[s, t], ss_sem.at[s, t])

    def start_states(s, inner):
        m0, m10, m2 = inner
        m210 = compose(m2, m10)
        zwait(s, 1, -1)
        behind = compose(zmap_if(s, -1), zmap_if(s, -2))
        early = apply_map(zmap_if(s, 2), zmap_if(s, 1)[1][E:])
        zwait(s, 3, -3, 4)
        behind = compose(behind, zmap_if(s, -3))
        early = apply_map(zmap_if(s, -4), apply_map(zmap_if(s, 3), early))
        here = apply_map(behind, early)
        ret_of = [here] + [apply_map(m, here) for m in (m0, m10, m210)]
        for t in range(NX):
            ret[s, t] = ret_of[t].astype(BF)
        spread(lambda t: rcopy(s, t, x), lambda t: rlocal(s, t))

    def unit(v):
        return v * lax.rsqrt(jnp.sum(v * v, axis=1, keepdims=True) + 1.0)

    gain = gain_ref[...]

    def final_parts(s):
        state = apply_map(zmap(s, 1), zmap(s, 0)[1][E:])
        for k in (2, 4, 6):
            state = apply_map(compose(zmap(s, k + 1), zmap(s, k)), state)
        place = lax.broadcasted_iota(jnp.int32, (HE, E), 1) == (
            lax.broadcasted_iota(jnp.int32, (HE, E), 0) + HE * side_half
        )
        memf = dot_tn(state.astype(BF), jnp.where(place, 1.0, 0.0).astype(BF))
        memory = memf.astype(BF)

        def pick(ref):
            row = ref[s].astype(F32)
            return jnp.where(head == 0, row[0:1, :], row[1:2, :])

        qn, kn, nv = unit(pick(nq_ref)), unit(pick(nk_ref)), pick(nv_ref)
        nbeta = jnp.where(head == 0, nbeta_ref[s, 0], nbeta_ref[s, 1])
        ndecay = jnp.where(head == 0, ndecay_ref[s, 0], ndecay_ref[s, 1])
        row = lax.broadcasted_iota(jnp.int32, (PAD, E), 0)
        asked = jnp.where(row == 0, qn, jnp.where(row == 1, kn, 0.0))
        seen = sum(dot(part, memory) for part in split3(asked))
        recall, retrieve = seen[0:1, :], seen[1:2, :]
        intersect = jnp.sum(kn * qn, axis=1, keepdims=True)
        lane = lax.broadcasted_iota(jnp.int32, (1, E), 1)
        nv = jnp.where((lane >= HE) == (side_half == 1), nv, 0.0)
        fresh = nv - ndecay * retrieve
        read = ndecay * recall + (nbeta * intersect) * fresh
        mine = memf[0:16, :]
        for k in range(1, NZ):
            mine = jnp.where(z == k, memf[16 * k : 16 * k + 16, :], mine)
        for t in range(NX):
            side[s, t, 0:4, :] = mine[4 * t : 4 * t + 4, :]
            side[s, t, 4:8, :] = jnp.broadcast_to(read, (4, E))
        spread(lambda t: scopy(s, t, x), lambda t: slocal(s, t))

    def outputs(s):
        collect(lambda t: rcopy(s, t, t), lambda t: rlocal(s, t))
        for h in heads:
            b = 2 * s + h
            start = jnp.concatenate([pin[s, 2 * h], pin[s, 2 * h + 1]], axis=0)
            o = lo[b] + dot_nt(reach[b], start)
            gate = head_of(s, 3, h).astype(F32)
            norm = lax.rsqrt(jnp.mean(o * o, axis=1, keepdims=True) + 0.001)
            out_ref[s, :, h * E : (h + 1) * E] = (
                o * norm * gain * (gate * jax.nn.sigmoid(gate))
            ).astype(BF)

    def last_parts(s):
        collect(lambda t: scopy(s, t, t), lambda t: slocal(s, t))
        for h in heads:
            both = sin[s, 2 * h] + sin[s, 2 * h + 1]
            cache_ref[s, h] = both[0:4].astype(BF)
            read = both[4:5]
            norm = lax.rsqrt(jnp.mean(read * read, axis=1, keepdims=True) + 0.001)
            first_ref[s : s + 1, h * E : (h + 1) * E] = read * norm * gain

    inner = []
    send_own(0)
    small_rows = jnp.concatenate(
        [wb_ref[...].astype(F32), wd_ref[...].astype(F32), jnp.zeros((PAD - 4, D), F32)], axis=0
    )
    wbd[...] = small_rows.T.astype(BF)
    forward(0)
    send_own(1)
    near_start(0)
    near_end(0)
    far_start(0)
    for cp in wcopies:
        cp.wait()
    part = near(0)
    forward(1)
    far_end(0)
    kept0 = chain_terms(0, far(0, part), lambda: near_start(1), lambda: far_start(1))
    xsend(0)
    near_end(1)
    part = near(1)
    far_end(1)
    kept1 = chain_terms(1, far(1, part), lambda: inner.append(zsend(0)), lambda: None)
    xsend(1)
    project(0, (0, 3))
    out_terms(0, *kept0)
    project(1, (0, 3))
    zrelay(0)
    out_terms(1, *kept1)
    inner.append(zsend(1))
    zrelay(1)
    start_states(0, inner[0])
    final_parts(0)
    start_states(1, inner[1])
    final_parts(1)
    outputs(0)
    last_parts(0)
    outputs(1)
    last_parts(1)

    for s in range(2):
        for half in range(2):
            for direction in range(2):
                ycopy(s, half, direction).wait_send()
        for direction in range(2):
            fcopy(s, direction).wait_send()
        for k in range(4):
            pcopy(s, k, c).wait_send()
        for t in range(NX):

            @pl.when(x != t)
            def _():
                xcopy(s, t, x).wait_send()
                rcopy(s, t, x).wait_send()
                scopy(s, t, x).wait_send()

        for hop in (2, -2, 1, -1):
            for piece in range(2):
                zcopy(s, z, piece, hop, hop).wait_send()
        for piece in range(2):
            for d in (1, -1):
                zcopy(s, z_at(-2 * d), piece, d, 3 * d).wait_send()
                if (piece == 0) == (d == 1):
                    zcopy(s, z_at(-2 * d), piece, 2 * d, 4).wait_send()


def hand_over(mixed_in, cache_in, first_in, mixed_out, cache_out, first_out, sems):
    pairs = ((mixed_in, mixed_out), (cache_in, cache_out), (first_in, first_out))
    copies = [pltpu.make_async_copy(a, b, sems.at[n]) for n, (a, b) in enumerate(pairs)]
    for cp in copies:
        cp.start()
    for cp in copies:
        cp.wait()


def shards(
    tokens,
    query_weight,
    key_weight,
    value_weight,
    gate_weight,
    beta_weight,
    decay_weight,
    beta_bias,
    rate_log,
    out_gain,
    new_query,
    new_key,
    new_value,
    new_beta,
    new_decay,
):
    smem = pl.BlockSpec(memory_space=pltpu.SMEM)
    vmem = pl.BlockSpec(memory_space=pltpu.VMEM)
    hbm = pl.BlockSpec(memory_space=pl.ANY)
    dma = pltpu.SemaphoreType.DMA
    out = pl.pallas_call(
        kernel,
        out_shape=(
            jax.ShapeDtypeStruct((2, L, 2 * E), BF),
            jax.ShapeDtypeStruct((2, 2, 4, E), BF),
            jax.ShapeDtypeStruct((2, 2 * E), F32),
        ),
        in_specs=[smem] * 4 + [hbm] * 5 + [vmem] * 6,
        out_specs=(vmem, vmem, vmem),
        scratch_shapes=[
            pltpu.VMEM((2, L, D), BF),
            pltpu.VMEM((4, D, 2 * E), BF),
            pltpu.VMEM((2, 4, L, 2 * E), BF),
            pltpu.VMEM((2, L, 2 * E), F32),
            pltpu.VMEM((D, PAD), BF),
            pltpu.VMEM((4, L, E), F32),
            pltpu.VMEM((4, L, E), BF),
            pltpu.VMEM((4, L, 2 * E), BF),
            pltpu.VMEM((2, 2, E + 2 * HE + PAD, E), BF),
            pltpu.VMEM((2, NX, ROWS, E), BF),
            pltpu.VMEM((2, NZ, ROWS, E), BF),
            pltpu.VMEM((2, NX, HE, E), BF),
            pltpu.VMEM((2, NX, HE, E), BF),
            pltpu.VMEM((2, NX, 8, E), F32),
            pltpu.VMEM((2, NX, 8, E), F32),
            dma((4,)),
            dma((2,)),
            dma((2, 2, 2)),
            dma((2, 2, 2)),
            dma((2, 2)),
            dma((2, 2)),
            dma((2, 4)),
            dma((2, 4)),
            dma((2, NX)),
            dma((2, NX)),
            dma((2, NZ, 2)),
            dma((2, NZ, 2)),
            dma((2, NX)),
            dma((2, NX)),
            dma((2, NX)),
            dma((2, NX)),
        ],
        compiler_params=pltpu.CompilerParams(
            collective_id=0, has_side_effects=True, vmem_limit_bytes=60 * 1024 * 1024
        ),
        name="delta_all",
    )(
        beta_bias,
        rate_log,
        new_beta,
        new_decay,
        tokens,
        query_weight,
        key_weight,
        value_weight,
        gate_weight,
        beta_weight.T,
        decay_weight.T,
        out_gain.reshape(1, E),
        new_query,
        new_key,
        new_value,
    )
    return pl.pallas_call(
        hand_over,
        out_shape=tuple(jax.ShapeDtypeStruct(o.shape, o.dtype) for o in out),
        in_specs=[hbm] * 3,
        out_specs=(vmem,) * 3,
        scratch_shapes=[dma((3,))],
        name="hand_over",
    )(*out)


def solution(mesh):
    torus = Mesh(mesh.devices.reshape(NZ, NX, NY, NC), ("z", "x", "y", "c"))
    sp, tp = ("z", "x"), ("y", "c")
    in_specs = (
        P(None, sp, tp),
        P(None, tp),
        P(None, tp),
        P(None, tp),
        P(None, tp),
        P(None, tp),
        P(None, tp),
        P(tp),
        P(tp),
        P(),
        P(None, tp, None),
        P(None, tp, None),
        P(None, tp, None),
        P(None, tp),
        P(None, tp),
    )
    out_specs = (P(None, sp, tp), P(None, tp, sp, None), P(None, tp))
    return jax.shard_map(
        shards, mesh=torus, in_specs=in_specs, out_specs=out_specs, check_vma=False
    )
```
